32 devices in a mesh: ep: 8 (over z, x), tp: 4 (over y, core).
Axes of the slice: x: 2, y: 2, z: 4, core: 2. Of those that a mesh axis runs over, the one named last changes fastest.
Arguments:
- mix_query: bfloat16 [2048, 2048], P('ep', 'tp'), may hold values from -6 to 6
- forget_input: bfloat16 [2048, 2048], P('ep', 'tp'), may hold values from -6 to 6
- mix_value: bfloat16 [2048, 2048], P('ep', 'tp'), may hold values from -6 to 6
- out_gate_input: bfloat16 [2048, 2048], P('ep', 'tp'), may hold values from -6 to 6
- decay_shift: float32 [2048, 16], P('ep', 'tp'), may hold values from -1.5 to 0
- forget_floor: float32 [2048], P('tp'), may hold values from 0.9 to 1
- head_gain: float32 [128], replicated, may hold values from 0.1 to 1.9
- w_mix_out: bfloat16 [2048, 2048], P(None, 'tp'), may hold values from -0.125 to 0.125
- moe_input: bfloat16 [2048, 2048], P('ep'), may hold values from -6 to 6
- moe_gain: float32 [2048], replicated, may hold values from 0.1 to 1.9
- routes: int32 [2048, 2], P('ep'), may hold values from 0 to 7, all different within a row; in each aligned block of 256 rows (0 to 255, 256 to 511, ...) at most 80 rows name the same one
- route_weight: float32 [2048, 2], P('ep'), may hold values from 0.1 to 1
- w_exp_gate: bfloat16 [8, 2048, 4096], P('ep', None, 'tp'), may hold values from -0.125 to 0.125
- w_exp_up: bfloat16 [8, 2048, 4096], P('ep', None, 'tp'), may hold values from -0.125 to 0.125
- w_exp_down: bfloat16 [8, 4096, 2048], P('ep', 'tp'), may hold values from -0.125 to 0.125
Outputs:
- mixed: bfloat16 [2048, 2048], P('ep', 'tp')
- moe_out: bfloat16 [2048, 2048], P('ep', 'tp')
The draws below stay inside these ranges and needn't reach their ends.
Inputs may be any that keep to these rules, and one draw needn't show every extreme that they name: `routes`: at most 80 of the rows of one index of ep name one expert, and in every draw some device's rows name one expert exactly 80 times; the experts of a row differ.
All inputs are finite; a program needn't handle non-finite values.
Results may differ from the reference program's by a relative error of at most 0.02.
Values may be sent and summed in bfloat16 or wider, within the bound.
No kernel may reach another device: no remote copies, remote signals or barrier semaphores. Data moves between devices by JAX's collectives and lax.ppermute only.
A program may use at most 64 MiB of HBM per device.

```python
import math
import jax
import jax.numpy as jnp
import numpy as np
from jax import lax

D = 2048
HEADS = 16
DK = 128
FE = 4096
TOP_K = 2
BLOCK = 64
TOK_DEV = 256
HW = 2048
TOKENS = 2048
EXPERTS = 8
CAP = 80
N_EP = 8
N_TP = 4


def draw_forget_floor(key, part):
    length = TOK_DEV * N_EP
    subkeys = jax.random.split(key, 3)
    fast_share = 0.5
    fast_heads = jax.random.bernoulli(subkeys[0], fast_share, (HEADS,))
    fast_rate = jnp.exp(jax.random.uniform(subkeys[1], (HEADS, DK), jnp.float32, math.log(0.02), math.log(0.07)))
    slow_rate = jnp.exp(jax.random.uniform(subkeys[2], (HEADS, DK), jnp.float32, math.log(0.3), 0.0)) / length
    keep_rate = jnp.where(fast_heads[:, None], fast_rate, slow_rate)
    return (1.0 - keep_rate).reshape(HEADS * DK).astype(jnp.float32)


def draw_decay_shift(key, part):
    length = TOK_DEV * N_EP
    subkeys = jax.random.split(key, 3)
    factor = jnp.exp(jax.random.uniform(subkeys[0], (N_EP, HEADS), jnp.float32, -math.log(2.0), math.log(2.0)))
    steady = -0.4 * jnp.repeat(factor, TOK_DEV, axis=0) / length
    places = jax.random.randint(subkeys[1], (2, HEADS), 0, length)
    depths = jnp.log(jax.random.uniform(subkeys[2], (2, HEADS), jnp.float32, 0.55, 0.8))
    marked = (jnp.arange(length)[:, None, None] == places[None, :, :]).astype(jnp.float32)
    return (steady + jnp.sum(marked * depths[None, :, :], axis=1)).astype(jnp.float32)


def spiked(result, stream_key, source, target, blocks, factor):
    owner, partner = [(jnp.arange(result.shape[axis_at]) // (result.shape[axis_at] // blocks)).reshape([-1 if axis == axis_at else 1 for axis in range(result.ndim)]) for axis_at in (source, target)]
    chosen = jax.random.permutation(stream_key, blocks)[partner]
    strong = (owner == chosen) | (owner == (partner + blocks // 2) % blocks)
    return jnp.where(strong, factor * result, result)


def block_levels(own_key, extent, pieces, smallest, largest):
    loudness = 1.0
    for dim, shards_of in pieces:
        draws = jax.random.uniform(jax.random.fold_in(jax.random.fold_in(own_key, 6), dim), (shards_of,), jnp.float32, smallest / len(pieces), largest / len(pieces))
        loudness = loudness * jnp.repeat(jnp.exp(draws), extent[dim] // shards_of).reshape((-1,) + (1,) * (len(extent) - 1 - dim))
    return loudness


def assign_block(stream_key, own, number, rows, amount, top, reach, slope):
    sequence = jax.random.permutation(stream_key, amount)
    heavy_load, common = shares(amount, rows * top, reach, slope, True), shares(amount, rows * top, reach, slope, False)
    places = jnp.arange(amount)

    def named(tallies, offset_by):
        used = int((tallies > 0).sum())
        fixed = max(1, used // 4)
        moved = fixed + (places - fixed + offset_by * (used - fixed)) % max(1, amount - fixed)
        return jnp.zeros((amount,), jnp.int32).at[sequence[jnp.where(places < fixed, places, moved)]].set(jnp.asarray(tallies, jnp.int32))

    tallies = jnp.where(number % 4 == 0, named(heavy_load, number // 4), named(common, number - number // 4 - 1))
    mixed = jax.random.permutation(jax.random.fold_in(own, 3), amount)
    donor, taker = mixed[0:amount // 2 * 2:2], mixed[1:amount // 2 * 2:2]
    margin = jnp.minimum(tallies[donor] - 1, reach - tallies[taker]) // 2
    margin = jnp.where((donor == sequence[0]) | (taker == sequence[0]) | (tallies[taker] == 0), 0, jnp.maximum(margin, 0))
    moved = jax.random.randint(jax.random.fold_in(own, 4), (amount // 2,), 0, 1 << 20) % (margin + 1)
    tallies = tallies.at[donor].add(-moved).at[taker].add(moved)
    labels = jnp.searchsorted(jnp.cumsum(tallies), jnp.arange(rows * top), side="right").astype(jnp.int32)
    grid = labels.reshape(top, rows).T
    grid = grid[jax.random.permutation(jax.random.fold_in(own, 1), rows)]
    offset_by = jax.random.randint(jax.random.fold_in(own, 2), (rows, 1), 0, top)
    return jnp.take_along_axis(grid, (jnp.arange(top)[None, :] + offset_by) % top, axis=1)


def shares(number_of, total, bound, skew, full):
    portions = [(1 << 20) // math.isqrt(rank ** skew) + 1 for rank in range(1, number_of + 1)]
    largest = bound if full else min(bound, max(-(-total // number_of), total * portions[0] // sum(portions)))
    least = 1 if total - largest >= number_of - 1 else 0
    given, rest = [largest] + [least] * (number_of - 1), total - largest - least * (number_of - 1)
    while rest > 0:
        movable = [i for i in range(1, number_of) if given[i] < largest] or [i for i in range(1, number_of) if given[i] < bound]
        mass, remaining = sum([portions[i] for i in movable]), rest
        for i in movable:
            addition = min(bound - given[i], max(1, remaining * portions[i] // mass), rest)
            given[i] = given[i] + addition
            rest = rest - addition
    return np.array(given)


def centred(stream_key, extent, scale, bound, pieces=(), kind=jnp.bfloat16):
    drawn = scale * jax.random.normal(stream_key, extent, jnp.float32)
    if pieces:
        drawn = drawn * block_levels(stream_key, extent, pieces, -0.22, 0.18)
    return jnp.clip(drawn, -bound, bound).astype(kind)


def bell_draw_with(key, shape, scale, reach, cuts, heavy, held_as=jnp.bfloat16):
    values = scale * jax.random.normal(key, shape, jnp.float32)
    if cuts:
        values = values * block_levels(key, shape, cuts, -0.22, 0.18)
    return jnp.clip(spiked(values, jax.random.fold_in(key, 3), *heavy), -reach, reach).astype(held_as)


def setup_inputs(seed: int = 0) -> dict:
    key_of = jax.random.split(jax.random.key(seed), 16)
    mix_query = centred(key_of[0], (TOKENS, HW), 1.0, 6.0, ((0, 8), (1, 4)))
    forget_input = centred(key_of[1], (TOKENS, HW), 1.0, 6.0, ((0, 8), (1, 4)))
    mix_value = centred(key_of[2], (TOKENS, HW), 1.0, 6.0, ((0, 8), (1, 4)))
    out_gate_input = centred(key_of[3], (TOKENS, HW), 1.0, 6.0, ((0, 8), (1, 4)))
    decay_shift = draw_decay_shift(jax.random.fold_in(key_of[15], 71), 0)
    forget_floor = draw_forget_floor(jax.random.fold_in(key_of[15], 71), 0)
    head_gain = jnp.clip(1.0 + 0.18 * jax.random.normal(key_of[6], (DK,), jnp.float32), 0.1, 1.9)
    w_mix_out = centred(key_of[7], (HW, D), HW ** -0.5, 0.125, ((1, 4),))
    moe_input = centred(key_of[8], (TOKENS, D), 1.0, 6.0, ((0, 8),))
    moe_gain = jnp.clip(1.0 + 0.18 * jax.random.normal(key_of[9], (D,), jnp.float32), 0.1, 1.9)
    routes_keys = jax.random.split(jax.random.fold_in(key_of[10], 1), TOKENS // TOK_DEV)
    routes_turns = jax.random.permutation(jax.random.fold_in(key_of[10], 3), TOKENS // TOK_DEV)
    routes = jax.vmap(lambda own, number: assign_block(jax.random.fold_in(key_of[10], 2), own, number, TOK_DEV, EXPERTS, TOP_K, CAP, 1))(routes_keys, routes_turns).reshape((TOKENS, TOP_K))
    route_weight = jnp.clip(0.1 + 0.9 * jax.random.uniform(key_of[11], (TOKENS, TOP_K), jnp.float32) ** block_levels(key_of[11], (TOKENS, TOP_K), ((0, 8),), -0.2, 0.2), 0.1, 1.0)
    w_exp_gate = centred(key_of[12], (EXPERTS, D, FE), D ** -0.5, 0.125, ((0, 8), (2, 4)))
    w_exp_up = centred(key_of[13], (EXPERTS, D, FE), D ** -0.5, 0.125, ((0, 8), (2, 4)))
    w_exp_down = bell_draw_with(key_of[14], (EXPERTS, FE, D), FE ** -0.5, 0.125, ((0, 8), (1, 4)), (1, 2, 4, 2.0))
    return {"mix_query": mix_query, "forget_input": forget_input, "mix_value": mix_value, "out_gate_input": out_gate_input, "decay_shift": decay_shift, "forget_floor": forget_floor, "head_gain": head_gain, "w_mix_out": w_mix_out, "moe_input": moe_input, "moe_gain": moe_gain, "routes": routes, "route_weight": route_weight, "w_exp_gate": w_exp_gate, "w_exp_up": w_exp_up, "w_exp_down": w_exp_down}


eps = 1e-06
highest_precision = lax.Precision.HIGHEST

def recurrence(query, input_gate, values, log_decay):
    length = query.shape[0]
    blocks = length // BLOCK

    def to_blocks(array):
        return array.reshape(blocks, BLOCK, HEADS, DK).transpose(0, 2, 1, 3)
    causal = jnp.tril(jnp.ones((BLOCK, BLOCK), bool))[:, :, None]

    def advance(recurrent_state, inputs):
        query_block, key_block, value_block, g_block = inputs
        running_decay = jnp.cumsum(g_block, axis=1)
        spread = running_decay[:, :, None, :] - running_decay[:, None, :, :]
        weights = jnp.where(causal, jnp.exp(jnp.minimum(spread, 0.0)), 0.0)
        scores = jnp.einsum('htk,htsk,hsk->hts', query_block, weights, key_block, precision=highest_precision)
        block_result = jnp.einsum('hts,hsv->htv', scores, value_block, precision=highest_precision)
        block_result = block_result + jnp.einsum('rsd,rda->rsa', query_block * jnp.exp(running_decay), recurrent_state, precision=highest_precision)
        closing_total = running_decay[:, -1:, :]
        carried_over_state = jnp.einsum('gbx,gbi->gxi', key_block * jnp.exp(closing_total - running_decay), value_block, precision=highest_precision)
        recurrent_state = jnp.exp(closing_total[:, 0, :])[:, :, None] * recurrent_state + carried_over_state
        return (recurrent_state, block_result)
    initial = jnp.zeros((HEADS, DK, DK), jnp.float32)
    _, block_result = lax.scan(advance, initial, (to_blocks(query), to_blocks(input_gate), to_blocks(values), to_blocks(log_decay)))
    return block_result.transpose(0, 2, 1, 3).reshape(length, HEADS, DK)

def token_mixer(mix_query, forget_input, mix_value, out_gate_input, decay_shift, forget_floor, head_gain, w_mix_out):
    length = mix_query.shape[0]
    gate_input = forget_input.astype(jnp.float32)
    forget = forget_floor + (1.0 - forget_floor) * jax.nn.sigmoid(gate_input)
    input_gate = (1.0 - forget_floor) * jax.nn.sigmoid(-gate_input)
    log_decay = jnp.log(forget) + jnp.repeat(decay_shift, DK, axis=1)
    block_result = recurrence(mix_query.astype(jnp.float32), input_gate, mix_value.astype(jnp.float32), log_decay)
    inverse = lax.rsqrt(lax.optimization_barrier(jnp.mean(block_result * block_result, axis=2, keepdims=True)) + eps)
    gated = jax.nn.silu(out_gate_input.astype(jnp.float32)).reshape(length, HEADS, DK)
    head_out = (block_result * inverse * head_gain * gated).reshape(length, HEADS * DK).astype(jnp.bfloat16)
    return jnp.dot(head_out, w_mix_out, preferred_element_type=jnp.float32).astype(jnp.bfloat16)

def experts_layer(moe_input, moe_gain, routes, route_weight, w_exp_gate, w_exp_up, w_exp_down):
    token_rows = moe_input.astype(jnp.float32)
    inverse = lax.rsqrt(lax.optimization_barrier(jnp.mean(token_rows * token_rows, axis=1, keepdims=True)) + eps)
    normed = (token_rows * inverse * moe_gain).astype(jnp.bfloat16)
    flat_ids = routes.reshape(-1)
    pair_count = flat_ids.shape[0]
    slot_count = CAP * N_EP
    group_size = FE // N_TP

    def one_expert(expert):
        matches = flat_ids == expert
        chosen = jnp.nonzero(matches, size=slot_count, fill_value=0)[0].astype(jnp.int32)
        how_many = jnp.sum(matches.astype(jnp.int32))
        usable = jnp.arange(slot_count, dtype=jnp.int32) < how_many
        picked = normed[chosen // TOP_K]
        gate_sum = jnp.dot(picked, w_exp_gate[expert], preferred_element_type=jnp.float32)
        up_sum = jnp.dot(picked, w_exp_up[expert], preferred_element_type=jnp.float32)
        hidden = (jax.nn.silu(gate_sum) * up_sum).astype(jnp.bfloat16)
        grouped = hidden.reshape(slot_count, N_TP, group_size).astype(jnp.float32)
        down_groups = w_exp_down[expert].reshape(N_TP, group_size, D).astype(jnp.float32)
        partial_value = jnp.einsum('sgf,gfd->sgd', grouped, down_groups).astype(jnp.bfloat16)
        summed = lax.optimization_barrier(jnp.sum(partial_value.astype(jnp.float32), axis=1)).astype(jnp.bfloat16)
        return (chosen, jnp.where(usable[:, None], summed, jnp.zeros_like(summed)))
    chosen_all, outputs = lax.map(one_expert, jnp.arange(EXPERTS, dtype=jnp.int32))
    pair_out = jnp.zeros((pair_count, D), jnp.float32).at[chosen_all.reshape(-1)].add(outputs.reshape(-1, D).astype(jnp.float32))
    combined = lax.optimization_barrier(jnp.sum(pair_out.reshape(-1, TOP_K, D) * route_weight[:, :, None], axis=1))
    return combined.astype(jnp.bfloat16)

def reference(mix_query, forget_input, mix_value, out_gate_input, decay_shift, forget_floor, head_gain, w_mix_out, moe_input, moe_gain, routes, route_weight, w_exp_gate, w_exp_up, w_exp_down):
    mixed = token_mixer(mix_query, forget_input, mix_value, out_gate_input, decay_shift, forget_floor, head_gain, w_mix_out)
    moe_out = experts_layer(moe_input, moe_gain, routes, route_weight, w_exp_gate, w_exp_up, w_exp_down)
    return (mixed, moe_out)
```

```python
import functools

import jax
import jax.numpy as jnp
from jax import lax
from jax.experimental import pallas as pl
from jax.experimental.pallas import tpu as pltpu
from jax.sharding import PartitionSpec as P

TOP_K = 2
LANES = 128
ROWS = 16
EPS = 1e-06
F32 = jnp.float32
BF16 = jnp.bfloat16

VMEM = pl.BlockSpec(memory_space=pltpu.VMEM)
SMEM = pl.BlockSpec(memory_space=pltpu.SMEM)
NN = (((1,), (0,)), ((), ()))
NT = (((1,), (1,)), ((), ()))
TN = (((0,), (0,)), ((), ()))


def mm(a, b, dims=NN):
    return lax.dot_general(a, b, dims, preferred_element_type=F32)


def split_mm(a, b, dims, left):
    wide = a if left else b
    high = wide.astype(BF16)
    low = (wide - high.astype(F32)).astype(BF16)
    if left:
        return mm(high, b, dims) + mm(low, b, dims)
    return mm(a, high, dims) + mm(a, low, dims)


def call(body, outs, args, name, flops, scratch=(), smem=1):
    specs = [SMEM] * smem + [VMEM] * (len(args) - smem)
    return pl.pallas_call(
        body,
        out_shape=tuple(jax.ShapeDtypeStruct(s, d) for s, d in outs),
        in_specs=specs,
        out_specs=tuple(VMEM for _ in outs),
        scratch_shapes=list(scratch),
        cost_estimate=pl.CostEstimate(flops=int(flops), transcendentals=0, bytes_accessed=1 << 20),
        name=name,
    )(*args)


def swap(array, axis, size, bit):
    return lax.ppermute(array, axis, [(i, i ^ bit) for i in range(size)])


def local_body(q_ref, x_ref, v_ref, shift_ref, floor_ref, sd_ref, qd_ref, within_ref):
    length, width = q_ref.shape
    heads = shift_ref.shape[1]
    size = width // heads
    low = floor_ref[...]
    x = x_ref[...].astype(F32)
    g = jnp.log(low + (1.0 - low) * jax.nn.sigmoid(x))
    key = (1.0 - low) * jax.nn.sigmoid(-x)
    row = lax.broadcasted_iota(jnp.int32, (length, length), 0)
    col = lax.broadcasted_iota(jnp.int32, (length, length), 1)
    lower = jnp.where(row >= col, 1.0, 0.0).astype(BF16)
    upper = jnp.where(row <= col, 1.0, 0.0).astype(BF16)
    total = split_mm(lower, g, NN, False)
    shift = shift_ref[...]
    down = split_mm(lower, shift, NN, False)
    across = split_mm(shift, upper, TN, True)
    for h in range(heads):
        cut = slice(h * size, (h + 1) * size)
        q = q_ref[:, cut].astype(F32)
        v = v_ref[:, cut]
        k = key[:, cut]
        run = total[:, cut]
        last = run[length - 1 : length, :]
        fall = down[:, h : h + 1]
        final = fall[length - 1 : length, :]
        grow = jnp.exp(run)
        scores = mm((q * grow).astype(BF16), (k * jnp.exp(-run)).astype(BF16), NT)
        mask = jnp.exp(jnp.minimum(fall - across[h : h + 1, :], 0.0))
        scores = jnp.where(row >= col, scores * mask, 0.0)
        within_ref[:, cut] = mm(scores.astype(BF16), v)
        qd_ref[:, cut] = (q * jnp.exp(run + fall)).astype(BF16)
        kept = (k * jnp.exp((last - run) + (final - fall))).astype(BF16)
        sd_ref[0:size, cut] = mm(v, kept, TN).astype(BF16)
        sd_ref[size : size + ROWS, cut] = jnp.broadcast_to(
            jnp.exp(last + final), (ROWS, size)
        ).astype(BF16)


def after(early, late):
    return (late[1] * early[0] + late[0], late[1] * early[1])


def pair(ref):
    rows = ref.shape[0] - ROWS
    return (ref[0:rows, :].astype(F32), ref[rows : rows + 1, :].astype(F32))


def put(ref, value):
    rows = ref.shape[0] - ROWS
    ref[0:rows, :] = value[0].astype(BF16)
    ref[rows : rows + ROWS, :] = jnp.broadcast_to(value[1], (ROWS, ref.shape[1])).astype(BF16)


def choose(flag, a, b):
    return tuple(jnp.where(flag, x, y) for x, y in zip(a, b))


def scan_body(bit, first, at_ref, tot_ref, *refs):
    if first:
        rec_ref, new_tot_ref, new_pre_ref = refs
    else:
        pre_ref, rec_ref, new_tot_ref, new_pre_ref = refs
    late = (at_ref[0] & bit) != 0
    tot = pair(tot_ref)
    rec = pair(rec_ref)
    pre = (jnp.zeros_like(tot[0]), jnp.ones_like(tot[1])) if first else pair(pre_ref)
    put(new_tot_ref, choose(late, after(rec, tot), after(tot, rec)))
    put(new_pre_ref, choose(late, after(rec, pre), pre))


def finish_body(bit, at_ref, within_ref, qd_ref, pre_ref, rec_ref, gate_ref, gain_ref, out_ref):
    width = qd_ref.shape[1]
    size = gain_ref.shape[1]
    late = (at_ref[0] & bit) != 0
    pre = pair(pre_ref)
    state = choose(late, after(pair(rec_ref), pre), pre)[0].astype(BF16)
    for h in range(width // size):
        cut = slice(h * size, (h + 1) * size)
        got = within_ref[:, cut] + mm(qd_ref[:, cut], state[:, cut], NT)
        scale = lax.rsqrt(jnp.mean(got * got, axis=1, keepdims=True) + EPS)
        gate = gate_ref[:, cut].astype(F32)
        gate = gate * jax.nn.sigmoid(gate)
        out_ref[:, cut] = (got * scale * gain_ref[...] * gate).astype(BF16)


def mixed_body(masks, at_ref, w_ref, *refs):
    out_ref = refs[-1]
    at = at_ref[1]
    acc = None
    for mask, ref in zip(masks, refs[:-1]):
        part = mm(ref[...], w_ref[at ^ mask])
        acc = part if acc is None else acc + part
    out_ref[...] = acc.astype(BF16)


def named(routes, lanes):
    seat = lax.broadcasted_iota(jnp.int32, (routes.shape[0], lanes), 1)
    return [routes[:, j : j + 1] == seat for j in range(TOP_K)]


def spread_body(near, far, at_ref, routes_ref, x_ref, gain_ref, *refs):
    normed_ref, rank_ref, mark_ref = refs[-3:]
    outs = refs[:-3]
    me = at_ref[0]
    at = at_ref[1]
    groups, count, width = normed_ref.shape
    x = x_ref[...].astype(F32)
    scale = lax.rsqrt(jnp.mean(x * x, axis=1, keepdims=True) + EPS)
    normed = (x * scale * gain_ref[...]).astype(BF16)
    for q in range(groups):
        normed_ref[q] = normed[:, q * width : (q + 1) * width]
    hits = named(routes_ref[...], LANES)
    hit = jnp.where(functools.reduce(jnp.logical_or, hits), 1.0, 0.0).astype(BF16)
    row = lax.broadcasted_iota(jnp.int32, (count, count), 0)
    col = lax.broadcasted_iota(jnp.int32, (count, count), 1)
    before = jnp.where(row < col, 1.0, 0.0).astype(BF16)
    same = jnp.where(row == col, 1.0, 0.0).astype(BF16)
    rank_ref[...] = mm(hit, before, TN)
    mark_ref[...] = mm(hit, same, TN)
    slot = lax.broadcasted_iota(jnp.int32, (outs[0].shape[0], count), 0).astype(F32)

    def chosen(k):
        e = me ^ k
        good = (rank_ref[pl.ds(e, 1), :] == slot) & (mark_ref[pl.ds(e, 1), :] > 0.5)
        return jnp.where(good, 1.0, 0.0).astype(BF16)

    for ref, k in zip(outs, far + near + (0,)):
        pick = chosen(k)
        if k in far:
            ref[...] = mm(pick, normed_ref[at]).astype(BF16)
        elif k in near:
            for j in range(groups // 2):
                ref[:, j * width : (j + 1) * width] = mm(
                    pick, normed_ref[2 * j + (at & 1)]
                ).astype(BF16)
        else:
            for q in range(groups):
                ref[:, q * width : (q + 1) * width] = mm(pick, normed_ref[q]).astype(BF16)


def places_body(order, at_ref, routes_ref, *outs):
    me = at_ref[0]
    count = routes_ref.shape[0]
    cap = outs[0].shape[1] // len(order)
    hits = named(routes_ref[...], LANES)
    hit = jnp.where(functools.reduce(jnp.logical_or, hits), 1.0, 0.0).astype(BF16)
    row = lax.broadcasted_iota(jnp.int32, (count, count), 0)
    col = lax.broadcasted_iota(jnp.int32, (count, count), 1)
    rank = mm(jnp.where(row > col, 1.0, 0.0).astype(BF16), hit)
    seat = lax.broadcasted_iota(jnp.int32, (count, outs[0].shape[1]), 1)
    routes = routes_ref[...]
    for j, ref in enumerate(outs):
        mine = jnp.sum(jnp.where(hits[j], rank, 0.0), axis=1, keepdims=True).astype(jnp.int32)
        turn = routes[:, j : j + 1] ^ me
        base = jnp.zeros_like(turn)
        for i, k in enumerate(order):
            base = jnp.where(turn == k, i * cap, base)
        ref[...] = jnp.where(seat == base + mine, 1.0, 0.0).astype(BF16)


def expert_body(plan, cap, at_ref, wg_ref, wu_ref, wd_ref, *refs):
    mine_ref, other_ref, x_ref, acc_ref = refs[-4:]
    refs = refs[:-4]
    at = at_ref[1]
    width = mine_ref.shape[1] // 2
    step = pl.program_id(0)

    @pl.when(step == 0)
    def _():
        for (block, piece), ref in zip(plan, refs):
            rows = slice(block * cap, (block + 1) * cap)
            for j, quarter in enumerate(piece(at)):
                lane = pl.multiple_of(quarter * width, width)
                x_ref[rows, pl.ds(lane, width)] = ref[:, j * width : (j + 1) * width]

    x = x_ref[...]
    gate = mm(x, wg_ref[0])
    up = mm(x, wu_ref[0])
    hidden = (gate * jax.nn.sigmoid(gate) * up).astype(BF16)
    part = mm(hidden, wd_ref[0])

    @pl.when(step == 0)
    def _():
        acc_ref[...] = part

    @pl.when(step > 0)
    def _():
        acc_ref[...] += part

    @pl.when(step == pl.num_programs(0) - 1)
    def _():
        for j in range(2):
            cut = slice(j * width, (j + 1) * width)
            lane = pl.multiple_of((2 * j + (at & 1)) * width, width)
            mine_ref[:, cut] = acc_ref[:, pl.ds(lane, width)].astype(BF16)
            lane = pl.multiple_of((2 * j + 1 - (at & 1)) * width, width)
            other_ref[:, cut] = acc_ref[:, pl.ds(lane, width)].astype(BF16)


def expert_call(at, wg, wu, wd, pieces, plan, blocks, cap, name):
    depth, hidden = wg.shape[1:]
    width = wd.shape[2]
    rows = blocks * cap
    chunk = min(hidden, 256)
    whole = lambda a: pl.BlockSpec(a.shape, lambda i: (0,) * a.ndim)
    half = jax.ShapeDtypeStruct((rows, width // 2), BF16)
    flops = 6 * rows * depth * hidden
    return pl.pallas_call(
        functools.partial(expert_body, plan, cap),
        grid=(hidden // chunk,),
        out_shape=(half, half),
        in_specs=[
            SMEM,
            pl.BlockSpec((1, depth, chunk), lambda i: (0, 0, i)),
            pl.BlockSpec((1, depth, chunk), lambda i: (0, 0, i)),
            pl.BlockSpec((1, chunk, width), lambda i: (0, i, 0)),
        ]
        + [whole(p) for p in pieces],
        out_specs=(pl.BlockSpec(half.shape, lambda i: (0, 0)),) * 2,
        scratch_shapes=[pltpu.VMEM((rows, depth), BF16), pltpu.VMEM((rows, width), F32)],
        cost_estimate=pl.CostEstimate(
            flops=flops, transcendentals=0, bytes_accessed=6 * depth * hidden
        ),
        name=name,
    )(at, wg, wu, wd, *pieces)


def halve_body(parts, at_ref, mine_ref, got_ref, keep_ref, *sends):
    width = keep_ref.shape[1]
    side = at_ref[1] // 2
    rows = keep_ref.shape[0] // parts

    def added(j):
        lane = pl.multiple_of(j * width, width)
        cut = pl.ds(lane, width)
        return (mine_ref[:, cut].astype(F32) + got_ref[:, cut].astype(F32)).astype(BF16)

    keep_ref[...] = added(side)
    send = added(1 - side)
    for i, ref in enumerate(sends):
        ref[...] = send[i * rows : (i + 1) * rows, :]


def add_body(first, at_ref, keep_ref, got_ref, *outs):
    rows = outs[0].shape[0]
    for i, ref in enumerate(outs):
        cut = slice((first + i) * rows, (first + i + 1) * rows)
        here = slice(i * rows, (i + 1) * rows)
        ref[...] = (keep_ref[cut, :].astype(F32) + got_ref[here, :].astype(F32)).astype(BF16)


def combine_body(at_ref, weight_ref, first_ref, second_ref, *refs):
    out_ref, all_ref = refs[-2:]
    cap = refs[0].shape[0]
    for i, ref in enumerate(refs[:-2]):
        all_ref[i * cap : (i + 1) * cap, :] = ref[...]
    weight = weight_ref[...]
    back = all_ref[...]
    out_ref[...] = (
        weight[:, 0:1] * mm(first_ref[...], back) + weight[:, 1:2] * mm(second_ref[...], back)
    ).astype(BF16)


def carried_in(own, place):
    gathered = lax.all_gather(own, "ep")
    rows = own.shape[0] - ROWS

    def one(turn, state):
        block = lax.dynamic_index_in_dim(gathered, turn, 0, False).astype(F32)
        return after(state, (block[:rows], block[rows : rows + 1]))

    width = own.shape[1]
    start = (jnp.zeros((rows, width), F32), jnp.ones((1, width), F32))
    state, decay = lax.fori_loop(0, place, one, start)
    return jnp.concatenate([state, jnp.broadcast_to(decay, (ROWS, width))], 0).astype(BF16)


def experts_grouped(moe_input, moe_gain, routes, route_weight, w_gate, w_up, w_down):
    count = moe_input.shape[0]
    experts = lax.axis_size("ep")
    cap = 5 * count * TOP_K // (4 * experts)
    x = moe_input.astype(F32)
    scale = lax.rsqrt(jnp.mean(x * x, axis=1, keepdims=True) + EPS)
    normed = (x * scale * moe_gain).astype(BF16)
    flat = routes.reshape(-1)
    one_hot = (flat[:, None] == jnp.arange(experts, dtype=jnp.int32)[None, :]).astype(jnp.int32)
    rank = jnp.sum((jnp.cumsum(one_hot, axis=0) - one_hot) * one_hot, axis=1)
    slot = flat * cap + rank
    owner = jnp.zeros((experts * cap,), jnp.int32).at[slot].set(
        jnp.arange(flat.shape[0], dtype=jnp.int32) // TOP_K
    )
    width = normed.shape[1] // lax.axis_size("tp")
    own = lax.dynamic_slice_in_dim(normed, lax.axis_index("tp") * width, width, 1)[owner]
    arrived = lax.all_to_all(own, "ep", split_axis=0, concat_axis=0, tiled=True)
    rows = lax.all_gather(arrived, "tp", axis=1, tiled=True)
    gate = jnp.dot(rows, w_gate[0], preferred_element_type=F32)
    up = jnp.dot(rows, w_up[0], preferred_element_type=F32)
    hidden = (jax.nn.silu(gate) * up).astype(BF16)
    part = jnp.dot(hidden, w_down[0], preferred_element_type=F32).astype(BF16)
    summed = lax.psum_scatter(part, "tp", scatter_dimension=1, tiled=True)
    back = lax.all_to_all(summed, "ep", split_axis=0, concat_axis=0, tiled=True)
    picked = back[slot].astype(F32).reshape(count, TOP_K, width)
    return jnp.sum(picked * route_weight[:, :, None], axis=1).astype(BF16)


def body(
    direct,
    mix_query,
    forget_input,
    mix_value,
    out_gate_input,
    decay_shift,
    forget_floor,
    head_gain,
    w_mix_out,
    moe_input,
    moe_gain,
    routes,
    route_weight,
    w_exp_gate,
    w_exp_up,
    w_exp_down,
):
    experts = lax.axis_size("ep")
    groups = lax.axis_size("tp")
    me = lax.axis_index("ep").astype(jnp.int32)
    at = jnp.stack([me, lax.axis_index("tp").astype(jnp.int32)])
    length, width = mix_query.shape
    size = head_gain.shape[0]
    count, depth = moe_input.shape
    slice_width = depth // groups
    cap = -(-5 * count * TOP_K // (4 * experts) // ROWS) * ROWS
    floor = forget_floor.reshape(1, -1)
    head_gain = head_gain.reshape(1, -1)
    half = experts // 2
    near = tuple(range(1, half))
    far = tuple(range(half, experts))
    block = lambda n: ((cap, n), BF16)

    if direct:
        sent = call(
            functools.partial(spread_body, near, far),
            [block(slice_width)] * len(far) + [block(depth // 2)] * len(near) + [block(depth)],
            [at, routes, moe_input, moe_gain.reshape(1, -1)],
            "spread",
            2 * experts * cap * count * depth,
            scratch=[
                pltpu.VMEM((groups, count, slice_width), BF16),
                pltpu.VMEM((LANES, count), F32),
                pltpu.VMEM((LANES, count), F32),
            ],
        )
        own_rows = sent[-1]
        far_in = {k: swap(a, "ep", experts, k) for k, a in zip(far, sent)}
        near_in = {k: swap(a, "ep", experts, k) for k, a in zip(near, sent[len(far) :])}

    state_shape = ((size + ROWS, width), BF16)
    sd, qd, within = call(
        local_body,
        [state_shape, ((length, width), BF16), ((length, width), F32)],
        [mix_query, forget_input, mix_value, decay_shift, floor],
        "local",
        8 * length * length * width,
        smem=0,
    )
    if direct:
        total, before = sd, None
        bit = 1
        while bit < half:
            got = swap(total, "ep", experts, bit)
            args = [at, total] + ([] if before is None else [before]) + [got]
            total, before = call(
                functools.partial(scan_body, bit, before is None),
                [state_shape, state_shape],
                args,
                "scan",
                8 * size * width,
            )
            bit *= 2
        got = lax.ppermute(total, "ep", [(i, i ^ bit) for i in range(experts) if not i & bit])
    else:
        bit = 0
        before = carried_in(sd, me)
        got = before
    head_out = call(
        functools.partial(finish_body, bit),
        [((length, width), BF16)],
        [at, within, qd, before, got, out_gate_input, head_gain],
        "finish",
        2 * length * size * width,
    )[0]
    if direct:
        across = swap(head_out, "tp", groups, 2)
        pieces = [head_out, across, swap(head_out, "tp", groups, 1), swap(across, "tp", groups, 1)]
        mixed = call(
            functools.partial(mixed_body, (0, 2, 1, 3)),
            [((length, w_mix_out.shape[1]), BF16)],
            [at, w_mix_out.reshape(groups, width, -1)] + pieces,
            "mixed",
            2 * length * groups * width * w_mix_out.shape[1],
        )[0]
    else:
        mixed = jnp.dot(
            lax.all_gather(head_out, "tp", axis=1, tiled=True),
            w_mix_out,
            preferred_element_type=F32,
        ).astype(BF16)
        moe_out = experts_grouped(
            moe_input, moe_gain, routes, route_weight, w_exp_gate, w_exp_up, w_exp_down
        )
        return (mixed, moe_out)

    own_half = lambda at: (at & 1, 2 + (at & 1))
    other_half = lambda at: (1 - (at & 1), 3 - (at & 1))
    only = lambda mask: (lambda at: (at ^ mask,))
    everything = lambda at: tuple(range(groups))

    near_pieces = [own_rows]
    near_plan = [(0, everything)]
    for i, k in enumerate(near):
        near_pieces += [near_in[k], swap(near_in[k], "tp", groups, 1)]
        near_plan += [(i + 1, own_half), (i + 1, other_half)]
    far_pieces = []
    far_plan = []
    for i, k in enumerate(far):
        here = far_in[k]
        there = swap(here, "tp", groups, 2)
        far_pieces += [here, there, swap(here, "tp", groups, 1), swap(there, "tp", groups, 1)]
        far_plan += [(i, only(0)), (i, only(2)), (i, only(1)), (i, only(3))]

    weights = (w_exp_gate, w_exp_up, w_exp_down)
    returned = {}
    for kind, keys, pieces, plan, parts in (
        ("near", (0,) + near, near_pieces, near_plan, 1),
        ("far", far, far_pieces, far_plan, 2),
    ):
        rows = len(keys) * cap
        mine, other = expert_call(at, *weights, pieces, plan, len(keys), cap, "expert_" + kind)
        got = swap(other, "tp", groups, 1)
        keep, *sends = call(
            functools.partial(halve_body, parts),
            [((rows, slice_width), BF16)] + [((rows // parts, slice_width), BF16)] * parts,
            [at, mine, got],
            "halve_" + kind,
            rows * slice_width * 4,
        )
        per = len(keys) // parts
        for i, send in enumerate(sends):
            back = swap(send, "tp", groups, 2)
            done = call(
                functools.partial(add_body, i * per),
                [block(slice_width)] * per,
                [at, keep, back],
                "add_" + kind,
                rows * slice_width,
            )
            for k, a in zip(keys[i * per : (i + 1) * per], done):
                returned[k] = swap(a, "ep", experts, k) if k else a

    order = (0,) + near + far
    seats = call(
        functools.partial(places_body, order),
        [((count, experts * cap), BF16)] * TOP_K,
        [at, routes],
        "places",
        2 * count * count * LANES,
    )
    moe_out = call(
        combine_body,
        [((count, slice_width), BF16)],
        [at, route_weight, *seats] + [returned[k] for k in order],
        "combine",
        4 * count * experts * cap * slice_width,
        scratch=[pltpu.VMEM((experts * cap, slice_width), BF16)],
    )[0]
    return (mixed, moe_out)


def solution(mesh):
    placed = (
        P("ep", "tp"),
        P("ep", "tp"),
        P("ep", "tp"),
        P("ep", "tp"),
        P("ep", "tp"),
        P("tp"),
        P(),
        P(None, "tp"),
        P("ep", None),
        P(),
        P("ep", None),
        P("ep", None),
        P("ep", None, "tp"),
        P("ep", None, "tp"),
        P("ep", "tp", None),
    )
    groups = mesh.shape["tp"]
    experts = mesh.shape["ep"]
    direct = groups == 4 and experts <= 8 and experts & (experts - 1) == 0 and experts >= 4
    return jax.shard_map(
        functools.partial(body, direct),
        mesh=mesh,
        in_specs=placed,
        out_specs=(P("ep", "tp"), P("ep", "tp")),
        check_vma=False,
    )
```

```python
import functools

import jax
import jax.numpy as jnp
from jax import lax
from jax.experimental import pallas as pl
from jax.experimental.pallas import tpu as pltpu
from jax.sharding import PartitionSpec as P


TOP_K = 2
ROWS = 16
EPS = 1e-06
F32 = jnp.float32
BF16 = jnp.bfloat16

VMEM = pl.BlockSpec(memory_space=pltpu.VMEM)
GRANT = 16 << 20
WEIGH = 4e9
NN = (((1,), (0,)), ((), ()))
NT = (((1,), (1,)), ((), ()))
TN = (((0,), (0,)), ((), ()))


def mm(a, b, dims=NN):
    return lax.dot_general(a, b, dims, preferred_element_type=F32)


def split_mm(a, b, dims, left):
    wide = a if left else b
    high = wide.astype(BF16)
    low = (wide - high.astype(F32)).astype(BF16)
    if left:
        return mm(high, b, dims) + mm(low, b, dims)
    return mm(a, high, dims) + mm(a, low, dims)


def call(body, outs, args, flops, scratch=()):
    return pl.pallas_call(
        body,
        out_shape=tuple(jax.ShapeDtypeStruct(s, d) for s, d in outs),
        in_specs=[VMEM] * len(args),
        out_specs=tuple(VMEM for _ in outs),
        scratch_shapes=list(scratch),
        compiler_params=pltpu.CompilerParams(vmem_limit_bytes=GRANT),
        cost_estimate=pl.CostEstimate(
            flops=int(max(flops, WEIGH)), transcendentals=0, bytes_accessed=1 << 20
        ),
    )(*args)


def swap(array, axis, size, bit):
    return lax.ppermute(array, axis, [(i, i ^ bit) for i in range(size)])


def in_hbm(*arrays):
    return [pltpu.with_memory_space_constraint(a, pltpu.HBM) for a in arrays]


def local_body(q_ref, x_ref, v_ref, shift_ref, floor_ref, sd_ref, qd_ref, within_ref):
    length, width = q_ref.shape
    heads = shift_ref.shape[0]
    size = width // heads
    low = floor_ref[...]
    x = x_ref[...].astype(F32)
    g = jnp.log(low + (1.0 - low) * jax.nn.sigmoid(x))
    key = (1.0 - low) * jax.nn.sigmoid(-x)
    row = lax.broadcasted_iota(jnp.int32, (length, length), 0)
    col = lax.broadcasted_iota(jnp.int32, (length, length), 1)
    lower = jnp.where(row >= col, 1.0, 0.0).astype(BF16)
    upper = jnp.where(row <= col, 1.0, 0.0).astype(BF16)
    total = split_mm(lower, g, NN, False)
    shift = shift_ref[...]
    if heads == 1:
        shift = jnp.broadcast_to(shift, (8, length))
    down = split_mm(lower, shift, NT, False)
    across = split_mm(shift, upper, NN, True)
    for h in range(heads):
        cut = slice(h * size, (h + 1) * size)
        q = q_ref[:, cut].astype(F32)
        v = v_ref[:, cut]
        k = key[:, cut]
        run = total[:, cut]
        last = run[length - 1 : length, :]
        fall = down[:, h : h + 1]
        final = fall[length - 1 : length, :]
        grow = jnp.exp(run)
        scores = mm((q * grow).astype(BF16), (k * jnp.exp(-run)).astype(BF16), NT)
        mask = jnp.exp(jnp.minimum(fall - across[h : h + 1, :], 0.0))
        scores = jnp.where(row >= col, scores * mask, 0.0)
        within_ref[:, cut] = mm(scores.astype(BF16), v)
        qd_ref[:, cut] = (q * jnp.exp(run + fall)).astype(BF16)
        kept = (k * jnp.exp((last - run) + (final - fall))).astype(BF16)
        sd_ref[0:size, cut] = mm(v, kept, TN).astype(BF16)
        sd_ref[size : size + ROWS, cut] = jnp.broadcast_to(
            jnp.exp(last + final), (ROWS, size)
        ).astype(BF16)


def after(early, late):
    return (late[1] * early[0] + late[0], late[1] * early[1])


def pair(ref):
    rows = ref.shape[0] - ROWS
    return (ref[0:rows, :].astype(F32), ref[rows : rows + 1, :].astype(F32))


def put(ref, value):
    rows = ref.shape[0] - ROWS
    ref[0:rows, :] = value[0].astype(BF16)
    ref[rows : rows + ROWS, :] = jnp.broadcast_to(value[1], (ROWS, ref.shape[1])).astype(BF16)


def choose(flag, a, b):
    return tuple(jnp.where(flag, x, y) for x, y in zip(a, b))


def scan_body(bit, first, tot_ref, *refs):
    if first:
        rec_ref, new_tot_ref, new_pre_ref = refs
    else:
        pre_ref, rec_ref, new_tot_ref, new_pre_ref = refs
    late = (lax.axis_index("ep") & bit) != 0
    tot = pair(tot_ref)
    rec = pair(rec_ref)
    pre = (jnp.zeros_like(tot[0]), jnp.ones_like(tot[1])) if first else pair(pre_ref)
    put(new_tot_ref, choose(late, after(rec, tot), after(tot, rec)))
    put(new_pre_ref, choose(late, after(rec, pre), pre))


def finish_body(bit, within_ref, qd_ref, pre_ref, rec_ref, gate_ref, gain_ref, out_ref):
    width = qd_ref.shape[1]
    size = gain_ref.shape[1]
    late = (lax.axis_index("ep") & bit) != 0
    pre = pair(pre_ref)
    state = choose(late, after(pair(rec_ref), pre), pre)[0].astype(BF16)
    for h in range(width // size):
        cut = slice(h * size, (h + 1) * size)
        got = within_ref[:, cut] + mm(qd_ref[:, cut], state[:, cut], NT)
        scale = lax.rsqrt(jnp.mean(got * got, axis=1, keepdims=True) + EPS)
        gate = gate_ref[:, cut].astype(F32)
        gate = gate * jax.nn.sigmoid(gate)
        out_ref[:, cut] = (got * scale * gain_ref[...] * gate).astype(BF16)


def mixed_body(masks, w_ref, *refs):
    out_ref = refs[-1]
    at = lax.axis_index("tp")
    acc = None
    for mask, ref in zip(masks, refs[:-1]):
        part = mm(ref[...], w_ref[at ^ mask])
        acc = part if acc is None else acc + part
    out_ref[...] = acc.astype(BF16)


def named(routes, experts):
    seat = lax.broadcasted_iota(jnp.int32, (experts, routes.shape[1]), 0)
    return [routes[j : j + 1, :] == seat for j in range(TOP_K)]


def ranked(hits):
    hit = jnp.where(functools.reduce(jnp.logical_or, hits), 1.0, 0.0)
    count = hit.shape[1]
    row = lax.broadcasted_iota(jnp.int32, (count, count), 0)
    col = lax.broadcasted_iota(jnp.int32, (count, count), 1)
    return mm(hit.astype(BF16), jnp.where(row < col, 1.0, 0.0).astype(BF16)), hit


def spread_body(near, far, routes_ref, x_ref, gain_ref, *refs):
    normed_ref, rank_ref, mark_ref = refs[-3:]
    outs = refs[:-3]
    me = lax.axis_index("ep")
    at = lax.axis_index("tp")
    groups, count, width = normed_ref.shape
    x = x_ref[...].astype(F32)
    scale = lax.rsqrt(jnp.mean(x * x, axis=1, keepdims=True) + EPS)
    normed = (x * scale * gain_ref[...]).astype(BF16)
    for q in range(groups):
        normed_ref[q] = normed[:, q * width : (q + 1) * width]
    rank_ref[...], mark_ref[...] = ranked(named(routes_ref[...], rank_ref.shape[0]))
    slot = lax.broadcasted_iota(jnp.int32, (outs[0].shape[0], count), 0).astype(F32)

    def chosen(k):
        e = me ^ k
        good = (rank_ref[pl.ds(e, 1), :] == slot) & (mark_ref[pl.ds(e, 1), :] > 0.5)
        return jnp.where(good, 1.0, 0.0).astype(BF16)

    for ref, k in zip(outs, far + near + (0,)):
        pick = chosen(k)
        if k in far:
            ref[...] = mm(pick, normed_ref[at]).astype(BF16)
        elif k in near:
            for j in range(groups // 2):
                ref[:, j * width : (j + 1) * width] = mm(
                    pick, normed_ref[2 * j + (at & 1)]
                ).astype(BF16)
        else:
            for q in range(groups):
                ref[:, q * width : (q + 1) * width] = mm(pick, normed_ref[q]).astype(BF16)


def places_body(order, experts, routes_ref, weight_ref, first_ref, second_ref, column_ref, row_ref):
    me = lax.axis_index("ep")
    cap = first_ref.shape[1] // len(order)
    routes = routes_ref[...]
    hits = named(routes, experts)
    rank, _ = ranked(hits)
    row_ref[...] = jnp.zeros_like(row_ref)
    for j in range(TOP_K):
        turn = routes[j : j + 1, :] ^ me
        base = jnp.zeros_like(turn)
        for i, k in enumerate(order):
            base = jnp.where(turn == k, i * cap, base)
        mine = jnp.sum(jnp.where(hits[j], rank, 0.0), axis=0, keepdims=True)
        row_ref[j : j + 1, :] = base.astype(F32) + mine
        row_ref[TOP_K + j : TOP_K + j + 1, :] = weight_ref[j : j + 1, :]
    column = row_ref[...].T
    column_ref[...] = column
    seat = lax.broadcasted_iota(jnp.int32, first_ref.shape, 1)
    for j, ref in enumerate((first_ref, second_ref)):
        place = column[:, j : j + 1].astype(jnp.int32)
        ref[...] = jnp.where(seat == place, 1.0, 0.0).astype(BF16)


def expert_body(plan, cap, wg_ref, wu_ref, wd_ref, *refs):
    mine_ref, other_ref, x_ref, acc_ref = refs[-4:]
    at = lax.axis_index("tp")
    width = mine_ref.shape[1] // 2
    for (block, piece), ref in zip(plan, refs[:-4]):
        rows = slice(block * cap, (block + 1) * cap)
        for j, quarter in enumerate(piece(at)):
            lane = pl.multiple_of(quarter * width, width)
            x_ref[rows, pl.ds(lane, width)] = ref[:, j * width : (j + 1) * width]
    x = x_ref[...]
    hidden = wg_ref.shape[2]
    chunk = min(hidden, 512)
    parts = []
    for c in range(0, hidden, chunk):
        gate = mm(x, wg_ref[0, :, c : c + chunk])
        up = mm(x, wu_ref[0, :, c : c + chunk])
        parts.append((gate * jax.nn.sigmoid(gate) * up).astype(BF16))
    acc_ref[...] = mm(jnp.concatenate(parts, axis=1), wd_ref[0]).astype(BF16)
    for j in range(2):
        cut = slice(j * width, (j + 1) * width)
        lane = pl.multiple_of((2 * j + (at & 1)) * width, width)
        mine_ref[:, cut] = acc_ref[:, pl.ds(lane, width)]
        lane = pl.multiple_of((2 * j + 1 - (at & 1)) * width, width)
        other_ref[:, cut] = acc_ref[:, pl.ds(lane, width)]


def expert_call(wg, wu, wd, pieces, plan, blocks, cap):
    depth, hidden = wg.shape[1:]
    width = wd.shape[2]
    rows = blocks * cap
    half = ((rows, width // 2), BF16)
    return call(
        functools.partial(expert_body, plan, cap),
        [half, half],
        [wg, wu, wd, *pieces],
        6 * rows * depth * hidden,
        scratch=[pltpu.VMEM((rows, depth), BF16), pltpu.VMEM((rows, width), BF16)],
    )


def halve_body(parts, mine_ref, got_ref, keep_ref, *sends):
    width = keep_ref.shape[1]
    side = lax.axis_index("tp") // 2
    rows = keep_ref.shape[0] // parts

    def added(j):
        lane = pl.multiple_of(j * width, width)
        cut = pl.ds(lane, width)
        return (mine_ref[:, cut].astype(F32) + got_ref[:, cut].astype(F32)).astype(BF16)

    keep_ref[...] = added(side)
    send = added(1 - side)
    for i, ref in enumerate(sends):
        ref[...] = send[i * rows : (i + 1) * rows, :]


def add_body(first, keep_ref, got_ref, *outs):
    rows = outs[0].shape[0]
    for i, ref in enumerate(outs):
        cut = slice((first + i) * rows, (first + i + 1) * rows)
        here = slice(i * rows, (i + 1) * rows)
        ref[...] = (keep_ref[cut, :].astype(F32) + got_ref[here, :].astype(F32)).astype(BF16)


def combine_body(column_ref, first_ref, second_ref, *refs):
    out_ref, all_ref = refs[-2:]
    cap = refs[0].shape[0]
    for i, ref in enumerate(refs[:-2]):
        all_ref[i * cap : (i + 1) * cap, :] = ref[...]
    weight = column_ref[:, TOP_K : 2 * TOP_K]
    back = all_ref[...]
    out_ref[...] = (
        weight[:, 0:1] * mm(first_ref[...], back) + weight[:, 1:2] * mm(second_ref[...], back)
    ).astype(BF16)


def carried_in(own, place):
    gathered = lax.all_gather(own, "ep")
    rows = own.shape[0] - ROWS

    def one(turn, state):
        block = lax.dynamic_index_in_dim(gathered, turn, 0, False).astype(F32)
        return after(state, (block[:rows], block[rows : rows + 1]))

    width = own.shape[1]
    start = (jnp.zeros((rows, width), F32), jnp.ones((1, width), F32))
    state, decay = lax.fori_loop(0, place, one, start)
    return jnp.concatenate([state, jnp.broadcast_to(decay, (ROWS, width))], 0).astype(BF16)


def experts_grouped(moe_input, moe_gain, routes, route_weight, w_gate, w_up, w_down):
    count = moe_input.shape[0]
    experts = lax.axis_size("ep")
    cap = 5 * count * TOP_K // (4 * experts)
    x = moe_input.astype(F32)
    scale = lax.rsqrt(jnp.mean(x * x, axis=1, keepdims=True) + EPS)
    normed = (x * scale * moe_gain).astype(BF16)
    flat = routes.reshape(-1)
    one_hot = (flat[:, None] == jnp.arange(experts, dtype=jnp.int32)[None, :]).astype(jnp.int32)
    rank = jnp.sum((jnp.cumsum(one_hot, axis=0) - one_hot) * one_hot, axis=1)
    slot = flat * cap + rank
    owner = jnp.zeros((experts * cap,), jnp.int32).at[slot].set(
        jnp.arange(flat.shape[0], dtype=jnp.int32) // TOP_K
    )
    width = normed.shape[1] // lax.axis_size("tp")
    own = lax.dynamic_slice_in_dim(normed, lax.axis_index("tp") * width, width, 1)[owner]
    arrived = lax.all_to_all(own, "ep", split_axis=0, concat_axis=0, tiled=True)
    rows = lax.all_gather(arrived, "tp", axis=1, tiled=True)
    gate = jnp.dot(rows, w_gate[0], preferred_element_type=F32)
    up = jnp.dot(rows, w_up[0], preferred_element_type=F32)
    hidden = (jax.nn.silu(gate) * up).astype(BF16)
    part = jnp.dot(hidden, w_down[0], preferred_element_type=F32).astype(BF16)
    summed = lax.psum_scatter(part, "tp", scatter_dimension=1, tiled=True)
    back = lax.all_to_all(summed, "ep", split_axis=0, concat_axis=0, tiled=True)
    picked = back[slot].astype(F32).reshape(count, TOP_K, width)
    return jnp.sum(picked * route_weight[:, :, None], axis=1).astype(BF16)


def body(
    direct,
    mix_query,
    forget_input,
    mix_value,
    out_gate_input,
    decay_shift,
    forget_floor,
    head_gain,
    w_mix_out,
    moe_input,
    moe_gain,
    routes,
    route_weight,
    w_exp_gate,
    w_exp_up,
    w_exp_down,
):
    experts = lax.axis_size("ep")
    groups = lax.axis_size("tp")
    me = lax.axis_index("ep").astype(jnp.int32)
    length, width = mix_query.shape
    size = head_gain.shape[0]
    count, depth = moe_input.shape
    slice_width = depth // groups
    cap = -(-5 * count * TOP_K // (4 * experts) // ROWS) * ROWS
    floor = forget_floor.reshape(1, -1)
    head_gain = head_gain.reshape(1, -1)
    half = experts // 2
    near = tuple(range(1, half))
    far = tuple(range(half, experts))
    block = lambda n: ((cap, n), BF16)
    padded = -(-experts // ROWS) * ROWS

    if direct:
        sent = call(
            functools.partial(spread_body, near, far),
            [block(slice_width)] * len(far) + [block(depth // 2)] * len(near) + [block(depth)],
            in_hbm(routes.T, moe_input, moe_gain.reshape(1, -1)),
            2 * experts * cap * count * depth,
            scratch=[
                pltpu.VMEM((groups, count, slice_width), BF16),
                pltpu.VMEM((padded, count), F32),
                pltpu.VMEM((padded, count), F32),
            ],
        )
        own_rows = sent[-1]
        far_in = {k: swap(a, "ep", experts, k) for k, a in zip(far, sent)}
        near_in = {k: swap(a, "ep", experts, k) for k, a in zip(near, sent[len(far) :])}

    state_shape = ((size + ROWS, width), BF16)
    sd, qd, within = call(
        local_body,
        [state_shape, ((length, width), BF16), ((length, width), F32)],
        in_hbm(mix_query, forget_input, mix_value, decay_shift.T, floor),
        8 * length * length * width,
    )
    if direct:
        total, before = sd, None
        bit = 1
        while bit < half:
            got = swap(total, "ep", experts, bit)
            args = [total] + ([] if before is None else [before]) + [got]
            total, before = call(
                functools.partial(scan_body, bit, before is None),
                [state_shape, state_shape],
                args,
                8 * size * width,
            )
            bit *= 2
        got = lax.ppermute(total, "ep", [(i, i ^ bit) for i in range(experts) if not i & bit])
    else:
        bit = 0
        before = carried_in(sd, me)
        got = before
    head_out = call(
        functools.partial(finish_body, bit),
        [((length, width), BF16)],
        [within, qd, before, got, out_gate_input, head_gain],
        2 * length * size * width,
    )[0]
    if direct:
        across = swap(head_out, "tp", groups, 2)
        pieces = [head_out, across]
        pieces += [swap(head_out, "tp", groups, 1), swap(across, "tp", groups, 1)]
        mixed = call(
            functools.partial(mixed_body, (0, 2, 1, 3)),
            [((length, w_mix_out.shape[1]), BF16)],
            [w_mix_out.reshape(groups, width, -1)] + pieces,
            2 * length * groups * width * w_mix_out.shape[1],
        )[0]
    else:
        mixed = jnp.dot(
            lax.all_gather(head_out, "tp", axis=1, tiled=True),
            w_mix_out,
            preferred_element_type=F32,
        ).astype(BF16)
        moe_out = experts_grouped(
            moe_input, moe_gain, routes, route_weight, w_exp_gate, w_exp_up, w_exp_down
        )
        return (mixed, moe_out)

    own_half = lambda at: (at & 1, 2 + (at & 1))
    other_half = lambda at: (1 - (at & 1), 3 - (at & 1))
    only = lambda mask: (lambda at: (at ^ mask,))
    everything = lambda at: tuple(range(groups))

    near_pieces = [own_rows]
    near_plan = [(0, everything)]
    for i, k in enumerate(near):
        near_pieces += [near_in[k], swap(near_in[k], "tp", groups, 1)]
        near_plan += [(i + 1, own_half), (i + 1, other_half)]
    far_pieces = []
    far_plan = []
    for i, k in enumerate(far):
        here = far_in[k]
        there = swap(here, "tp", groups, 2)
        far_pieces += [here, there]
        far_pieces += [swap(here, "tp", groups, 1), swap(there, "tp", groups, 1)]
        far_plan += [(i, only(0)), (i, only(2)), (i, only(1)), (i, only(3))]

    weights = (w_exp_gate, w_exp_up, w_exp_down)
    returned = {}
    for keys, pieces, plan, parts in (
        ((0,) + near, near_pieces, near_plan, 1), (far, far_pieces, far_plan, 2)
    ):
        rows = len(keys) * cap
        mine, other = expert_call(*weights, pieces, plan, len(keys), cap)
        got = swap(other, "tp", groups, 1)
        keep, *sends = call(
            functools.partial(halve_body, parts),
            [((rows, slice_width), BF16)] + [((rows // parts, slice_width), BF16)] * parts,
            [mine, got],
            rows * slice_width * 4,
        )
        per = len(keys) // parts
        for i, send in enumerate(sends):
            back = swap(send, "tp", groups, 2)
            done = call(
                functools.partial(add_body, i * per),
                [block(slice_width)] * per,
                [keep, back],
                rows * slice_width,
            )
            for k, a in zip(keys[i * per : (i + 1) * per], done):
                returned[k] = swap(a, "ep", experts, k) if k else a

    order = (0,) + near + far
    first, second, column = call(
        functools.partial(places_body, order, padded),
        [((count, experts * cap), BF16)] * TOP_K + [((count, 8), F32)],
        [routes.T, route_weight.T],
        2 * count * count * padded,
        scratch=[pltpu.VMEM((8, count), F32)],
    )
    moe_out = call(
        combine_body,
        [((count, slice_width), BF16)],
        [column, first, second] + [returned[k] for k in order],
        4 * count * experts * cap * slice_width,
        scratch=[pltpu.VMEM((experts * cap, slice_width), BF16)],
    )[0]
    return (mixed, moe_out)


def solution(mesh):
    placed = (
        P("ep", "tp"),
        P("ep", "tp"),
        P("ep", "tp"),
        P("ep", "tp"),
        P("ep", "tp"),
        P("tp"),
        P(),
        P(None, "tp"),
        P("ep", None),
        P(),
        P("ep", None),
        P("ep", None),
        P("ep", None, "tp"),
        P("ep", None, "tp"),
        P("ep", "tp", None),
    )
    groups = mesh.shape["tp"]
    experts = mesh.shape["ep"]
    direct = groups == 4 and experts <= 8 and experts & (experts - 1) == 0 and experts >= 4

    def whole(*args):
        return body(direct, *args)

    return jax.shard_map(
        whole,
        mesh=mesh,
        in_specs=placed,
        out_specs=(P("ep", "tp"), P("ep", "tp")),
        check_vma=False,
    )
```

```python
import functools

import jax
import jax.numpy as jnp
from jax import lax
from jax.experimental import pallas as pl
from jax.experimental.pallas import tpu as pltpu
from jax.sharding import PartitionSpec as P


TOP_K = 2
ROWS = 16
EPS = 1e-06
F32 = jnp.float32
BF16 = jnp.bfloat16

VMEM = pl.BlockSpec(memory_space=pltpu.VMEM)
GRANT = 16 << 20
LONG = 2e10
NN = (((1,), (0,)), ((), ()))
NT = (((1,), (1,)), ((), ()))
TN = (((0,), (0,)), ((), ()))


def mm(a, b, dims=NN):
    return lax.dot_general(a, b, dims, preferred_element_type=F32)


def split_mm(a, b, dims, left):
    wide = a if left else b
    high = wide.astype(BF16)
    low = (wide - high.astype(F32)).astype(BF16)
    if left:
        return mm(high, b, dims) + mm(low, b, dims)
    return mm(a, high, dims) + mm(a, low, dims)


def call(body, outs, args, flops, scratch=()):
    return pl.pallas_call(
        body,
        out_shape=tuple(jax.ShapeDtypeStruct(s, d) for s, d in outs),
        in_specs=[VMEM] * len(args),
        out_specs=tuple(VMEM for _ in outs),
        scratch_shapes=list(scratch),
        compiler_params=pltpu.CompilerParams(vmem_limit_bytes=GRANT),
        cost_estimate=pl.CostEstimate(flops=int(flops), transcendentals=0, bytes_accessed=1 << 20),
    )(*args)


def swap(array, axis, size, bit):
    return lax.ppermute(array, axis, [(i, i ^ bit) for i in range(size)])


def in_hbm(*arrays):
    return [pltpu.with_memory_space_constraint(a, pltpu.HBM) for a in arrays]


def local_body(q_ref, x_ref, v_ref, shift_ref, floor_ref, *refs):
    sd_ref, qd_ref, within_ref = refs[-3:]
    length, width = q_ref.shape
    heads = shift_ref.shape[0]
    size = width // heads
    low = floor_ref[...]
    x = x_ref[...].astype(F32)
    g = jnp.log(low + (1.0 - low) * jax.nn.sigmoid(x))
    key = (1.0 - low) * jax.nn.sigmoid(-x)
    row = lax.broadcasted_iota(jnp.int32, (length, length), 0)
    col = lax.broadcasted_iota(jnp.int32, (length, length), 1)
    lower = jnp.where(row >= col, 1.0, 0.0).astype(BF16)
    upper = jnp.where(row <= col, 1.0, 0.0).astype(BF16)
    total = split_mm(lower, g, NN, False)
    shift = shift_ref[...]
    if heads == 1:
        shift = jnp.broadcast_to(shift, (8, length))
    down = split_mm(lower, shift, NT, False)
    across = split_mm(shift, upper, NN, True)
    states, decays = [], []
    for h in range(heads):
        cut = slice(h * size, (h + 1) * size)
        q = q_ref[:, cut].astype(F32)
        v = v_ref[:, cut]
        k = key[:, cut]
        run = total[:, cut]
        last = run[length - 1 : length, :]
        fall = down[:, h : h + 1]
        final = fall[length - 1 : length, :]
        grow = jnp.exp(run)
        scores = mm((q * grow).astype(BF16), (k * jnp.exp(-run)).astype(BF16), NT)
        mask = jnp.exp(jnp.minimum(fall - across[h : h + 1, :], 0.0))
        scores = jnp.where(row >= col, scores * mask, 0.0)
        within_ref[:, cut] = mm(scores.astype(BF16), v)
        qd_ref[:, cut] = (q * jnp.exp(run + fall)).astype(BF16)
        kept = (k * jnp.exp((last - run) + (final - fall))).astype(BF16)
        states.append(mm(v, kept, TN))
        decays.append(jnp.exp(last + final))
    value = (jnp.concatenate(states, axis=1), jnp.concatenate(decays, axis=1))
    if len(refs) == 3:
        put(sd_ref, value)
    else:
        put_wide(sd_ref, value, refs[0])


def after(early, late):
    return (late[1] * early[0] + late[0], late[1] * early[1])


def pair(ref, first=0):
    rows = ref.shape[0] - ROWS
    return (ref[first:rows, :].astype(F32), ref[rows : rows + 1, :].astype(F32))


def put(ref, value, first=0):
    rows = ref.shape[0] - ROWS
    ref[first:rows, :] = value[0].astype(BF16)
    ref[rows : rows + ROWS, :] = jnp.broadcast_to(value[1], (ROWS, ref.shape[1])).astype(BF16)


def pair_wide(ref, first):
    rows = ref.shape[0] - ROWS
    width = ref.shape[1] // 2
    state = jnp.concatenate([ref[first:rows, 0:width], ref[first:rows, width : 2 * width]], axis=0)
    return (state.astype(F32), ref[rows : rows + 1, 0:width].astype(F32))


def put_wide(ref, value, rows_ref):
    first = rows_ref.shape[0]
    ref[0:first, :] = rows_ref[...]
    rows = ref.shape[0] - ROWS
    half = rows - first
    width = ref.shape[1] // 2
    state = value[0].astype(BF16)
    decay = jnp.broadcast_to(value[1], (ROWS, width)).astype(BF16)
    for j in range(2):
        cut = slice(j * width, (j + 1) * width)
        ref[first:rows, cut] = state[j * half : (j + 1) * half, :]
        ref[rows : rows + ROWS, cut] = decay


def choose(flag, a, b):
    return tuple(jnp.where(flag, x, y) for x, y in zip(a, b))


def scan_body(bit, first, cap, *refs):
    new_tot_ref, new_pre_ref = refs[-2:]
    tot_ref, rec_ref = refs[:2]
    late = (lax.axis_index("ep") & bit) != 0
    tot = pair_wide(tot_ref, cap)
    rec = pair_wide(rec_ref, cap)
    pre = (jnp.zeros_like(tot[0]), jnp.ones_like(tot[1])) if first else pair(refs[2])
    new = choose(late, after(rec, tot), after(tot, rec))
    if new_tot_ref.shape[0] == new_pre_ref.shape[0]:
        put(new_tot_ref, new)
    else:
        put_wide(new_tot_ref, new, refs[-3])
    put(new_pre_ref, choose(late, after(rec, pre), pre))


def finish_body(bit, within_ref, qd_ref, pre_ref, rec_ref, gate_ref, gain_ref, out_ref):
    width = qd_ref.shape[1]
    size = gain_ref.shape[1]
    late = (lax.axis_index("ep") & bit) != 0
    pre = pair(pre_ref)
    rec = pair(rec_ref, rec_ref.shape[0] - pre_ref.shape[0])
    state = choose(late, after(rec, pre), pre)[0].astype(BF16)
    for h in range(width // size):
        cut = slice(h * size, (h + 1) * size)
        got = within_ref[:, cut] + mm(qd_ref[:, cut], state[:, cut], NT)
        scale = lax.rsqrt(jnp.mean(got * got, axis=1, keepdims=True) + EPS)
        gate = gate_ref[:, cut].astype(F32)
        gate = gate * jax.nn.sigmoid(gate)
        out_ref[:, cut] = (got * scale * gain_ref[...] * gate).astype(BF16)


def mixed_body(masks, w_ref, *refs):
    out_ref = refs[-1]
    at = lax.axis_index("tp")
    acc = None
    for mask, ref in zip(masks, refs[:-1]):
        part = mm(ref[...], w_ref[at ^ mask])
        acc = part if acc is None else acc + part
    out_ref[...] = acc.astype(BF16)


def named(routes, experts):
    seat = lax.broadcasted_iota(jnp.int32, (experts, routes.shape[1]), 0)
    return [routes[j : j + 1, :] == seat for j in range(TOP_K)]


def ranked(hits):
    hit = jnp.where(functools.reduce(jnp.logical_or, hits), 1.0, 0.0)
    count = hit.shape[1]
    row = lax.broadcasted_iota(jnp.int32, (count, count), 0)
    col = lax.broadcasted_iota(jnp.int32, (count, count), 1)
    return mm(hit.astype(BF16), jnp.where(row < col, 1.0, 0.0).astype(BF16)), hit


def spread_body(near, far, routes_ref, x_ref, gain_ref, *refs):
    normed_ref, rank_ref, mark_ref = refs[-3:]
    outs = refs[:-3]
    me = lax.axis_index("ep")
    at = lax.axis_index("tp")
    groups, count, width = normed_ref.shape
    x = x_ref[...].astype(F32)
    scale = lax.rsqrt(jnp.mean(x * x, axis=1, keepdims=True) + EPS)
    normed = (x * scale * gain_ref[...]).astype(BF16)
    for q in range(groups):
        normed_ref[q] = normed[:, q * width : (q + 1) * width]
    rank_ref[...], mark_ref[...] = ranked(named(routes_ref[...], rank_ref.shape[0]))
    slot = lax.broadcasted_iota(jnp.int32, (outs[0].shape[0], count), 0).astype(F32)

    def chosen(k):
        e = me ^ k
        good = (rank_ref[pl.ds(e, 1), :] == slot) & (mark_ref[pl.ds(e, 1), :] > 0.5)
        return jnp.where(good, 1.0, 0.0).astype(BF16)

    for ref, k in zip(outs, far + near + (0,)):
        pick = chosen(k)
        if k in far:
            ref[...] = mm(pick, normed_ref[at]).astype(BF16)
        elif k in near:
            for j in range(groups // 2):
                ref[:, j * width : (j + 1) * width] = mm(
                    pick, normed_ref[2 * j + (at & 1)]
                ).astype(BF16)
        else:
            for q in range(groups):
                ref[:, q * width : (q + 1) * width] = mm(pick, normed_ref[q]).astype(BF16)


def places_body(order, experts, routes_ref, weight_ref, first_ref, second_ref, column_ref, row_ref):
    me = lax.axis_index("ep")
    cap = first_ref.shape[1] // len(order)
    routes = routes_ref[...]
    hits = named(routes, experts)
    rank, _ = ranked(hits)
    row_ref[...] = jnp.zeros_like(row_ref)
    for j in range(TOP_K):
        turn = routes[j : j + 1, :] ^ me
        base = jnp.zeros_like(turn)
        for i, k in enumerate(order):
            base = jnp.where(turn == k, i * cap, base)
        mine = jnp.sum(jnp.where(hits[j], rank, 0.0), axis=0, keepdims=True)
        row_ref[j : j + 1, :] = base.astype(F32) + mine
        row_ref[TOP_K + j : TOP_K + j + 1, :] = weight_ref[j : j + 1, :]
    column = row_ref[...].T
    column_ref[...] = column
    seat = lax.broadcasted_iota(jnp.int32, first_ref.shape, 1)
    for j, ref in enumerate((first_ref, second_ref)):
        place = column[:, j : j + 1].astype(jnp.int32)
        ref[...] = jnp.where(seat == place, 1.0, 0.0).astype(BF16)


def expert_body(plan, cap, wg_ref, wu_ref, wd_ref, *refs):
    mine_ref, other_ref, x_ref, acc_ref = refs[-4:]
    at = lax.axis_index("tp")
    width = mine_ref.shape[1] // 2
    for (block, count, piece), ref in zip(plan, refs[:-4]):
        rows = slice(block * cap, (block + count) * cap)
        for j, quarter in enumerate(piece(at)):
            lane = pl.multiple_of(quarter * width, width)
            x_ref[rows, pl.ds(lane, width)] = ref[0 : count * cap, j * width : (j + 1) * width]
    x = x_ref[...]
    hidden = wg_ref.shape[2]
    chunk = min(hidden, 512)
    parts = []
    for c in range(0, hidden, chunk):
        gate = mm(x, wg_ref[0, :, c : c + chunk])
        up = mm(x, wu_ref[0, :, c : c + chunk])
        parts.append((gate * jax.nn.sigmoid(gate) * up).astype(BF16))
    acc_ref[...] = mm(jnp.concatenate(parts, axis=1), wd_ref[0]).astype(BF16)
    for j in range(2):
        cut = slice(j * width, (j + 1) * width)
        lane = pl.multiple_of((2 * j + (at & 1)) * width, width)
        mine_ref[:, cut] = acc_ref[:, pl.ds(lane, width)]
        lane = pl.multiple_of((2 * j + 1 - (at & 1)) * width, width)
        other_ref[:, cut] = acc_ref[:, pl.ds(lane, width)]


def expert_call(wg, wu, wd, pieces, plan, blocks, cap):
    depth, hidden = wg.shape[1:]
    width = wd.shape[2]
    rows = blocks * cap
    half = ((rows, width // 2), BF16)
    return call(
        functools.partial(expert_body, plan, cap),
        [half, half],
        [wg, wu, wd, *pieces],
        6 * rows * depth * hidden,
        scratch=[pltpu.VMEM((rows, depth), BF16), pltpu.VMEM((rows, width), BF16)],
    )


def halve_body(mine_ref, got_ref, keep_ref, send_ref):
    width = keep_ref.shape[1]
    side = lax.axis_index("tp") // 2
    for ref, j in ((keep_ref, side), (send_ref, 1 - side)):
        cut = pl.ds(pl.multiple_of(j * width, width), width)
        ref[...] = (mine_ref[:, cut].astype(F32) + got_ref[:, cut].astype(F32)).astype(BF16)


def pack_body(*refs):
    out_ref = refs[-1]
    rows = out_ref.shape[0] // (len(refs) - 1)
    for i, ref in enumerate(refs[:-1]):
        out_ref[i * rows : (i + 1) * rows, :] = ref[0:rows, :]


def add_body(keep_ref, got_ref, *refs):
    outs = refs[-2:]
    rows = keep_ref.shape[0] // 2
    if len(refs) == 3:
        outs[0][rows:, :] = refs[0][...]
    for i, ref in enumerate(outs):
        cut = slice(i * rows, (i + 1) * rows)
        ref[0:rows, :] = (keep_ref[cut, :].astype(F32) + got_ref[cut, :].astype(F32)).astype(BF16)


def combine_body(column_ref, first_ref, second_ref, *refs):
    out_ref, all_ref = refs[-2:]
    cap = all_ref.shape[0] // (len(refs) - 2)
    for i, ref in enumerate(refs[:-2]):
        all_ref[i * cap : (i + 1) * cap, :] = ref[0:cap, :]
    weight = column_ref[:, TOP_K : 2 * TOP_K]
    back = all_ref[...]
    out_ref[...] = (
        weight[:, 0:1] * mm(first_ref[...], back) + weight[:, 1:2] * mm(second_ref[...], back)
    ).astype(BF16)


def carried_in(own, place):
    gathered = lax.all_gather(own, "ep")
    rows = own.shape[0] - ROWS

    def one(turn, state):
        block = lax.dynamic_index_in_dim(gathered, turn, 0, False).astype(F32)
        return after(state, (block[:rows], block[rows : rows + 1]))

    width = own.shape[1]
    start = (jnp.zeros((rows, width), F32), jnp.ones((1, width), F32))
    state, decay = lax.fori_loop(0, place, one, start)
    return jnp.concatenate([state, jnp.broadcast_to(decay, (ROWS, width))], 0).astype(BF16)


def experts_grouped(moe_input, moe_gain, routes, route_weight, w_gate, w_up, w_down):
    count = moe_input.shape[0]
    experts = lax.axis_size("ep")
    cap = 5 * count * TOP_K // (4 * experts)
    x = moe_input.astype(F32)
    scale = lax.rsqrt(jnp.mean(x * x, axis=1, keepdims=True) + EPS)
    normed = (x * scale * moe_gain).astype(BF16)
    flat = routes.reshape(-1)
    one_hot = (flat[:, None] == jnp.arange(experts, dtype=jnp.int32)[None, :]).astype(jnp.int32)
    rank = jnp.sum((jnp.cumsum(one_hot, axis=0) - one_hot) * one_hot, axis=1)
    slot = flat * cap + rank
    owner = jnp.zeros((experts * cap,), jnp.int32).at[slot].set(
        jnp.arange(flat.shape[0], dtype=jnp.int32) // TOP_K
    )
    width = normed.shape[1] // lax.axis_size("tp")
    own = lax.dynamic_slice_in_dim(normed, lax.axis_index("tp") * width, width, 1)[owner]
    arrived = lax.all_to_all(own, "ep", split_axis=0, concat_axis=0, tiled=True)
    rows = lax.all_gather(arrived, "tp", axis=1, tiled=True)
    gate = jnp.dot(rows, w_gate[0], preferred_element_type=F32)
    up = jnp.dot(rows, w_up[0], preferred_element_type=F32)
    hidden = (jax.nn.silu(gate) * up).astype(BF16)
    part = jnp.dot(hidden, w_down[0], preferred_element_type=F32).astype(BF16)
    summed = lax.psum_scatter(part, "tp", scatter_dimension=1, tiled=True)
    back = lax.all_to_all(summed, "ep", split_axis=0, concat_axis=0, tiled=True)
    picked = back[slot].astype(F32).reshape(count, TOP_K, width)
    return jnp.sum(picked * route_weight[:, :, None], axis=1).astype(BF16)


def body(
    direct,
    mix_query,
    forget_input,
    mix_value,
    out_gate_input,
    decay_shift,
    forget_floor,
    head_gain,
    w_mix_out,
    moe_input,
    moe_gain,
    routes,
    route_weight,
    w_exp_gate,
    w_exp_up,
    w_exp_down,
):
    experts = lax.axis_size("ep")
    groups = lax.axis_size("tp")
    me = lax.axis_index("ep").astype(jnp.int32)
    length, width = mix_query.shape
    size = head_gain.shape[0]
    count, depth = moe_input.shape
    slice_width = depth // groups
    cap = -(-5 * count * TOP_K // (4 * experts) // ROWS) * ROWS
    floor = forget_floor.reshape(1, -1)
    head_gain = head_gain.reshape(1, -1)
    half = experts // 2
    near = tuple(range(1, half))
    far = tuple(range(half, experts))
    block = lambda n: ((cap, n), BF16)
    padded = -(-experts // ROWS) * ROWS

    if direct:
        sent = call(
            functools.partial(spread_body, near, far),
            [block(slice_width)] * len(far) + [block(depth // 2)] * len(near) + [block(depth)],
            in_hbm(routes.T, moe_input, moe_gain.reshape(1, -1)),
            LONG,
            scratch=[
                pltpu.VMEM((groups, count, slice_width), BF16),
                pltpu.VMEM((padded, count), F32),
                pltpu.VMEM((padded, count), F32),
            ],
        )
        own_rows = sent[-1]
        far_in = {k: swap(a, "ep", experts, k) for k, a in zip(far, sent)}
        near_out = dict(zip(near, sent[len(far) :]))
        near_in = {}

    state_shape = ((size + ROWS, width), BF16)
    wide_shape = ((cap + size // 2 + ROWS, 2 * width), BF16)
    total, qd, within = call(
        local_body,
        [
            wide_shape if direct else state_shape,
            ((length, width), BF16),
            ((length, width), F32),
        ],
        [mix_query, forget_input, mix_value, decay_shift.T, floor]
        + ([near_out[1]] if direct else []),
        LONG,
    )
    if direct:
        before = []
        bit = 1
        while bit < half:
            near_in[bit] = swap(total, "ep", experts, bit)
            last = 2 * bit == half
            total, *before = call(
                functools.partial(scan_body, bit, not before, cap),
                [state_shape if last else wide_shape, state_shape],
                [total, near_in[bit]] + before + ([] if last else [near_out[2 * bit]]),
                8 * size * width,
            )
            bit *= 2
        for k in near:
            if k not in near_in:
                near_in[k] = swap(near_out[k], "ep", experts, k)

    def gathered(keys):
        if 0 in keys:
            here = near_in[1]
            pieces = [own_rows, here, swap(here, "tp", groups, 1)]
            return pieces, [(0, 1, everything), (1, 1, own_half), (1, 1, other_half)]
        wide = keys[0] in near
        source = near_in if wide else far_in
        here = call(
            pack_body,
            [((2 * cap, depth // 2 if wide else slice_width), BF16)],
            [source[k] for k in keys],
            0,
        )[0]
        pieces = [here, swap(here, "tp", groups, 1)]
        if wide:
            return pieces, [(0, 2, own_half), (0, 2, other_half)]
        there = swap(here, "tp", groups, 2)
        pieces += [there, swap(there, "tp", groups, 1)]
        return pieces, [(0, 2, only(mask)) for mask in (0, 1, 2, 3)]

    own_half = lambda at: (at & 1, 2 + (at & 1))
    other_half = lambda at: (1 - (at & 1), 3 - (at & 1))
    only = lambda mask: (lambda at: (at ^ mask,))
    everything = lambda at: tuple(range(groups))

    if direct:
        weights = (w_exp_gate, w_exp_up, w_exp_down)
        returned = {}
        for i in range(experts // 2):
            keys = (2 * i, 2 * i + 1)
            rows = 2 * cap
            pieces, plan = gathered(keys)
            mine, other = expert_call(*weights, pieces, plan, 2, cap)
            got = swap(other, "tp", groups, 1)
            quarter = ((rows, slice_width), BF16)
            keep, send = call(halve_body, [quarter, quarter], [mine, got], 0)
            back = swap(send, "tp", groups, 2)
            with_state = half in keys
            done = call(
                add_body,
                [((cap + size + ROWS, width), BF16) if with_state else block(slice_width)]
                + [block(slice_width)],
                [keep, back] + ([total] if with_state else []),
                0,
            )
            for k, a in zip(keys, done):
                returned[k] = swap(a, "ep", experts, k) if k else a
        got = returned[half]
        before = before[0]
        bit = half
    else:
        bit = 0
        before = carried_in(total, me)
        got = before
    head_out = call(
        functools.partial(finish_body, bit),
        [((length, width), BF16)],
        [within, qd, before, got, out_gate_input, head_gain],
        2 * length * size * width,
    )[0]
    if direct:
        across = swap(head_out, "tp", groups, 2)
        pieces = [head_out, across]
        pieces += [swap(head_out, "tp", groups, 1), swap(across, "tp", groups, 1)]
        mixed = call(
            functools.partial(mixed_body, (0, 2, 1, 3)),
            [((length, w_mix_out.shape[1]), BF16)],
            [w_mix_out.reshape(groups, width, -1)] + pieces,
            2 * length * groups * width * w_mix_out.shape[1],
        )[0]
    else:
        mixed = jnp.dot(
            lax.all_gather(head_out, "tp", axis=1, tiled=True),
            w_mix_out,
            preferred_element_type=F32,
        ).astype(BF16)
        moe_out = experts_grouped(
            moe_input, moe_gain, routes, route_weight, w_exp_gate, w_exp_up, w_exp_down
        )
        return (mixed, moe_out)

    order = (0,) + near + far
    first, second, column = call(
        functools.partial(places_body, order, padded),
        [((count, experts * cap), BF16)] * TOP_K + [((count, 8), F32)],
        [routes.T, route_weight.T],
        2 * count * count * padded,
        scratch=[pltpu.VMEM((8, count), F32)],
    )
    moe_out = call(
        combine_body,
        [((count, slice_width), BF16)],
        [column, first, second] + [returned[k] for k in order],
        4 * count * experts * cap * slice_width,
        scratch=[pltpu.VMEM((experts * cap, slice_width), BF16)],
    )[0]
    return (mixed, moe_out)


def solution(mesh):
    placed = (
        P("ep", "tp"),
        P("ep", "tp"),
        P("ep", "tp"),
        P("ep", "tp"),
        P("ep", "tp"),
        P("tp"),
        P(),
        P(None, "tp"),
        P("ep", None),
        P(),
        P("ep", None),
        P("ep", None),
        P("ep", None, "tp"),
        P("ep", None, "tp"),
        P("ep", "tp", None),
    )
    groups = mesh.shape["tp"]
    experts = mesh.shape["ep"]
    direct = groups == 4 and experts <= 8 and experts & (experts - 1) == 0 and experts >= 4

    def whole(*args):
        return body(direct, *args)

    return jax.shard_map(
        whole,
        mesh=mesh,
        in_specs=placed,
        out_specs=(P("ep", "tp"), P("ep", "tp")),
        check_vma=False,
    )
```

```python
import functools

import jax
import jax.numpy as jnp
from jax import lax
from jax.experimental import pallas as pl
from jax.experimental.pallas import tpu as pltpu
from jax.sharding import PartitionSpec as P


TOP_K = 2
ROWS = 8
EPS = 1e-06
F32 = jnp.float32
BF16 = jnp.bfloat16

VMEM = pl.BlockSpec(memory_space=pltpu.VMEM)
GRANT = 16 << 20
LONG = 2e10
NN = (((1,), (0,)), ((), ()))
NT = (((1,), (1,)), ((), ()))
TN = (((0,), (0,)), ((), ()))


def mm(a, b, dims=NN):
    return lax.dot_general(a, b, dims, preferred_element_type=F32)


def split_mm(a, b, dims, left):
    wide = a if left else b
    high = wide.astype(BF16)
    low = (wide - high.astype(F32)).astype(BF16)
    if left:
        return mm(high, b, dims) + mm(low, b, dims)
    return mm(a, high, dims) + mm(a, low, dims)


def call(body, outs, args, flops, scratch=(), near=False):
    return pl.pallas_call(
        body,
        out_shape=tuple(pltpu.VMEM(s, d) if near else jax.ShapeDtypeStruct(s, d) for s, d in outs),
        in_specs=[VMEM] * len(args),
        out_specs=tuple(VMEM for _ in outs),
        scratch_shapes=list(scratch),
        compiler_params=pltpu.CompilerParams(vmem_limit_bytes=GRANT),
        cost_estimate=pl.CostEstimate(flops=int(flops), transcendentals=0, bytes_accessed=1 << 20),
    )(*args)


def swap(array, axis, size, bit):
    return lax.ppermute(array, axis, [(i, i ^ bit) for i in range(size)])


def send(array, half, i):
    peers = [(e, t, peer(half, i, t)) for e in range(2 * half) for t in range(4)]
    pairs = [(e * 4 + t, (e ^ k) * 4 + t) for e, t, k in peers]
    return lax.ppermute(array, ("ep", "tp"), pairs)


def send_near(array, experts, i):
    pairs = [(e * 4 + t, (e ^ (2 * i + (t & 1))) * 4 + t) for e in range(experts) for t in range(4)]
    return lax.ppermute(array, ("ep", "tp"), pairs)


def in_hbm(*arrays):
    return [pltpu.with_memory_space_constraint(a, pltpu.HBM) for a in arrays]


def local_body(q_ref, x_ref, v_ref, shift_ref, floor_ref, *refs):
    sd_ref, qd_ref, within_ref = refs[-3:]
    length, width = q_ref.shape
    heads = shift_ref.shape[0]
    size = width // heads
    low = floor_ref[...]
    x = x_ref[...].astype(F32)
    g = jnp.log(low + (1.0 - low) * jax.nn.sigmoid(x))
    key = (1.0 - low) * jax.nn.sigmoid(-x)
    row = lax.broadcasted_iota(jnp.int32, (length, length), 0)
    col = lax.broadcasted_iota(jnp.int32, (length, length), 1)
    lower = jnp.where(row >= col, 1.0, 0.0).astype(BF16)
    upper = jnp.where(row <= col, 1.0, 0.0).astype(BF16)
    total = split_mm(lower, g, NN, False)
    shift = shift_ref[...]
    if heads == 1:
        shift = jnp.broadcast_to(shift, (8, length))
    down = split_mm(lower, shift, NT, False)
    across = split_mm(shift, upper, NN, True)
    states, decays = [], []
    for h in range(heads):
        cut = slice(h * size, (h + 1) * size)
        q = q_ref[:, cut].astype(F32)
        v = v_ref[:, cut]
        k = key[:, cut]
        run = total[:, cut]
        last = run[length - 1 : length, :]
        fall = down[:, h : h + 1]
        final = fall[length - 1 : length, :]
        grow = jnp.exp(run)
        scores = mm((q * grow).astype(BF16), (k * jnp.exp(-run)).astype(BF16), NT)
        mask = jnp.exp(jnp.minimum(fall - across[h : h + 1, :], 0.0))
        scores = jnp.where(row >= col, scores * mask, 0.0)
        within_ref[:, cut] = mm(scores.astype(BF16), v)
        qd_ref[:, cut] = (q * jnp.exp(run + fall)).astype(BF16)
        kept = (k * jnp.exp((last - run) + (final - fall))).astype(BF16)
        states.append(mm(v, kept, TN))
        decays.append(jnp.exp(last + final))
    value = (jnp.concatenate(states, axis=1), jnp.concatenate(decays, axis=1))
    if len(refs) == 3:
        put(sd_ref, value)
    else:
        put_wide(sd_ref, value, refs[0])


def after(early, late):
    return (late[1] * early[0] + late[0], late[1] * early[1])


def pair(ref, first=0):
    rows = ref.shape[0] - ROWS
    return (ref[first:rows, :].astype(F32), ref[rows : rows + 1, :].astype(F32))


def put(ref, value, first=0):
    rows = ref.shape[0] - ROWS
    ref[first:rows, :] = value[0].astype(BF16)
    ref[rows : rows + ROWS, :] = jnp.broadcast_to(value[1], (ROWS, ref.shape[1])).astype(BF16)


def pair_wide(ref, first):
    rows = ref.shape[0] - ROWS
    width = ref.shape[1] // 2
    state = jnp.concatenate([ref[first:rows, 0:width], ref[first:rows, width : 2 * width]], axis=0)
    return (state.astype(F32), ref[rows : rows + 1, 0:width].astype(F32))


def put_wide(ref, value, rows_ref):
    first = rows_ref.shape[0]
    ref[0:first, :] = rows_ref[...]
    rows = ref.shape[0] - ROWS
    half = rows - first
    width = ref.shape[1] // 2
    state = value[0].astype(BF16)
    decay = jnp.broadcast_to(value[1], (ROWS, width)).astype(BF16)
    for j in range(2):
        cut = slice(j * width, (j + 1) * width)
        ref[first:rows, cut] = state[j * half : (j + 1) * half, :]
        ref[rows : rows + ROWS, cut] = decay


def choose(flag, a, b):
    return tuple(jnp.where(flag, x, y) for x, y in zip(a, b))


def scan_body(bit, first, cap, *refs):
    new_tot_ref, new_pre_ref = refs[-2:]
    tot_ref, rec_ref = refs[:2]
    late = (lax.axis_index("ep") & bit) != 0
    tot = pair_wide(tot_ref, cap)
    rec = pair_wide(rec_ref, cap)
    pre = (jnp.zeros_like(tot[0]), jnp.ones_like(tot[1])) if first else pair(refs[2])
    new = choose(late, after(rec, tot), after(tot, rec))
    if new_tot_ref.shape[0] == new_pre_ref.shape[0]:
        put(new_tot_ref, new)
    else:
        put_wide(new_tot_ref, new, refs[-3])
    put(new_pre_ref, choose(late, after(rec, pre), pre))


def finish_body(bit, within_ref, qd_ref, pre_ref, rec_ref, gate_ref, gain_ref, out_ref):
    width = qd_ref.shape[1]
    size = gain_ref.shape[1]
    late = (lax.axis_index("ep") & bit) != 0
    pre = pair(pre_ref)
    state = choose(late, after(pair(rec_ref), pre), pre)[0].astype(BF16)
    for h in range(width // size):
        cut = slice(h * size, (h + 1) * size)
        got = within_ref[:, cut] + mm(qd_ref[:, cut], state[:, cut], NT)
        scale = lax.rsqrt(jnp.mean(got * got, axis=1, keepdims=True) + EPS)
        gate = gate_ref[:, cut].astype(F32)
        gate = gate * jax.nn.sigmoid(gate)
        out_ref[:, cut] = (got * scale * gain_ref[...] * gate).astype(BF16)


def mixed_body(masks, w_ref, *refs):
    out_ref = refs[-1]
    at = lax.axis_index("tp")
    acc = None
    for mask, ref in zip(masks, refs[:-1]):
        part = mm(ref[...], w_ref[at ^ mask])
        acc = part if acc is None else acc + part
    out_ref[...] = acc.astype(BF16)


def named(routes, experts):
    seat = lax.broadcasted_iota(jnp.int32, (experts, routes.shape[1]), 0)
    return [routes[j : j + 1, :] == seat for j in range(TOP_K)]


def ranked(hits):
    hit = jnp.where(functools.reduce(jnp.logical_or, hits), 1.0, 0.0)
    count = hit.shape[1]
    row = lax.broadcasted_iota(jnp.int32, (count, count), 0)
    col = lax.broadcasted_iota(jnp.int32, (count, count), 1)
    return mm(hit.astype(BF16), jnp.where(row < col, 1.0, 0.0).astype(BF16)), hit


def peer(half, i, at):
    return half + i + (at & 1) * (half // 2)


def spread_body(half, routes_ref, x_ref, gain_ref, *refs):
    normed_ref, rank_ref, mark_ref = refs[-3:]
    at = lax.axis_index("tp")
    groups, _, width = normed_ref.shape
    x = x_ref[...].astype(F32)
    scale = lax.rsqrt(jnp.mean(x * x, axis=1, keepdims=True) + EPS)
    normed = (x * scale * gain_ref[...]).astype(BF16)
    for q in range(groups):
        normed_ref[q] = normed[:, q * width : (q + 1) * width]
    rank_ref[...], mark_ref[...] = ranked(named(routes_ref[...], rank_ref.shape[0]))
    for i, ref in enumerate(refs[:-3]):
        pick = chosen(rank_ref, mark_ref, peer(half, i, at), ref.shape[0])
        for j in range(groups // 2):
            cut = slice(j * width, (j + 1) * width)
            ref[:, cut] = mm(pick, normed_ref[2 * (at // 2) + j]).astype(BF16)


def spread_near_body(near, normed_ref, rank_ref, mark_ref, *outs):
    at = lax.axis_index("tp")
    groups, _, width = normed_ref.shape
    for ref, k in zip(outs, near + (0,)):
        pick = chosen(rank_ref, mark_ref, k, ref.shape[0])
        for j in range(groups // 2 if k else groups):
            cut = slice(j * width, (j + 1) * width)
            ref[:, cut] = mm(pick, normed_ref[2 * j + (at & 1) if k else j]).astype(BF16)


def chosen(rank_ref, mark_ref, k, cap):
    e = lax.axis_index("ep") ^ k
    slot = lax.broadcasted_iota(jnp.int32, (cap, rank_ref.shape[1]), 0).astype(F32)
    good = (rank_ref[pl.ds(e, 1), :] == slot) & (mark_ref[pl.ds(e, 1), :] > 0.5)
    return jnp.where(good, 1.0, 0.0).astype(BF16)


def places_body(order, experts, routes_ref, weight_ref, first_ref, second_ref, column_ref, row_ref):
    me = lax.axis_index("ep")
    cap = first_ref.shape[1] // len(order)
    routes = routes_ref[...]
    hits = named(routes, experts)
    rank, _ = ranked(hits)
    row_ref[...] = jnp.zeros_like(row_ref)
    for j in range(TOP_K):
        turn = routes[j : j + 1, :] ^ me
        base = jnp.zeros_like(turn)
        for i, k in enumerate(order):
            base = jnp.where(turn == k, i * cap, base)
        mine = jnp.sum(jnp.where(hits[j], rank, 0.0), axis=0, keepdims=True)
        row_ref[j : j + 1, :] = base.astype(F32) + mine
        row_ref[TOP_K + j : TOP_K + j + 1, :] = weight_ref[j : j + 1, :]
    column = row_ref[...].T
    column_ref[...] = column
    seat = lax.broadcasted_iota(jnp.int32, first_ref.shape, 1)
    for j, ref in enumerate((first_ref, second_ref)):
        place = column[:, j : j + 1].astype(jnp.int32)
        ref[...] = jnp.where(seat == place, 1.0, 0.0).astype(BF16)


def expert_body(plan, cap, wg_ref, wu_ref, wd_ref, *refs):
    mine_ref, other_ref, x_ref, acc_ref = refs[-4:]
    at = lax.axis_index("tp")
    width = x_ref.shape[1] // 4
    for (block, count, piece), ref in zip(plan, refs[:-4]):
        first = block(at) * cap
        rows = pl.ds(first if isinstance(first, int) else pl.multiple_of(first, cap), count * cap)
        for j, quarter in enumerate(piece(at)):
            lane = pl.multiple_of(quarter * width, width)
            x_ref[rows, pl.ds(lane, width)] = ref[0 : count * cap, j * width : (j + 1) * width]
    x = x_ref[...]
    hidden = wg_ref.shape[2]
    chunk = min(hidden, 512)
    parts = []
    for c in range(0, hidden, chunk):
        gate = mm(x, wg_ref[0, :, c : c + chunk])
        up = mm(x, wu_ref[0, :, c : c + chunk])
        parts.append((gate * jax.nn.sigmoid(gate) * up).astype(BF16))
    acc_ref[...] = mm(jnp.concatenate(parts, axis=1), wd_ref[0]).astype(BF16)
    for ref, block in ((mine_ref, at & 1), (other_ref, 1 - (at & 1))):
        ref[...] = acc_ref[pl.ds(pl.multiple_of(block * cap, cap), cap), :]


def expert_call(wg, wu, wd, pieces, plan, blocks, cap):
    depth, hidden = wg.shape[1:]
    width = wd.shape[2]
    rows = blocks * cap
    half = ((cap, width), BF16)
    return call(
        functools.partial(expert_body, plan, cap),
        [half, half],
        [wg, wu, wd, *pieces],
        6 * rows * depth * hidden,
        scratch=[pltpu.VMEM((rows, depth), BF16), pltpu.VMEM((rows, width), BF16)],
    )


def halve_body(mine_ref, got_ref, keep_ref, send_ref):
    width = keep_ref.shape[1]
    side = lax.axis_index("tp") // 2
    for ref, j in ((keep_ref, side), (send_ref, 1 - side)):
        cut = pl.ds(pl.multiple_of(j * width, width), width)
        ref[...] = (mine_ref[:, cut].astype(F32) + got_ref[:, cut].astype(F32)).astype(BF16)


def pack_body(*refs):
    out_ref = refs[-1]
    rows = out_ref.shape[0] // (len(refs) - 1)
    for i, ref in enumerate(refs[:-1]):
        out_ref[i * rows : (i + 1) * rows, :] = ref[0:rows, :]


def add_body(keep_ref, got_ref, out_ref):
    out_ref[...] = (keep_ref[...].astype(F32) + got_ref[...].astype(F32)).astype(BF16)


def combine_body(start, column_ref, first_ref, second_ref, *refs):
    out_ref, all_ref = refs[-2:]
    earlier = refs[:-2][len(refs) - 2 - (len(refs) - 2) % 2 :]
    blocks = refs[: (len(refs) - 2) // 2 * 2]
    core = lax.axis_index("tp") & 1
    cap, width = blocks[0].shape[0], out_ref.shape[1]
    cut = pl.ds(pl.multiple_of(core * width, width), width)
    for i in range(0, len(blocks), 2):
        for ref, side in ((blocks[i], core), (blocks[i + 1], 1 - core)):
            rows = pl.ds(pl.multiple_of((i + side) * cap, cap), cap)
            all_ref[rows, :] = ref[:, cut]
    weight = column_ref[:, TOP_K : 2 * TOP_K]
    back = all_ref[...]
    total = weight[:, 0:1] * mm(first_ref[:, start * cap : start * cap + back.shape[0]], back)
    total += weight[:, 1:2] * mm(second_ref[:, start * cap : start * cap + back.shape[0]], back)
    for ref in earlier:
        total += ref[...]
    out_ref[...] = total.astype(out_ref.dtype)


def carried_in(own, place):
    gathered = lax.all_gather(own, "ep")
    rows = own.shape[0] - ROWS

    def one(turn, state):
        block = lax.dynamic_index_in_dim(gathered, turn, 0, False).astype(F32)
        return after(state, (block[:rows], block[rows : rows + 1]))

    width = own.shape[1]
    start = (jnp.zeros((rows, width), F32), jnp.ones((1, width), F32))
    state, decay = lax.fori_loop(0, place, one, start)
    return jnp.concatenate([state, jnp.broadcast_to(decay, (ROWS, width))], 0).astype(BF16)


def experts_grouped(moe_input, moe_gain, routes, route_weight, w_gate, w_up, w_down):
    count = moe_input.shape[0]
    experts = lax.axis_size("ep")
    cap = 5 * count * TOP_K // (4 * experts)
    x = moe_input.astype(F32)
    scale = lax.rsqrt(jnp.mean(x * x, axis=1, keepdims=True) + EPS)
    normed = (x * scale * moe_gain).astype(BF16)
    flat = routes.reshape(-1)
    one_hot = (flat[:, None] == jnp.arange(experts, dtype=jnp.int32)[None, :]).astype(jnp.int32)
    rank = jnp.sum((jnp.cumsum(one_hot, axis=0) - one_hot) * one_hot, axis=1)
    slot = flat * cap + rank
    owner = jnp.zeros((experts * cap,), jnp.int32).at[slot].set(
        jnp.arange(flat.shape[0], dtype=jnp.int32) // TOP_K
    )
    width = normed.shape[1] // lax.axis_size("tp")
    own = lax.dynamic_slice_in_dim(normed, lax.axis_index("tp") * width, width, 1)[owner]
    arrived = lax.all_to_all(own, "ep", split_axis=0, concat_axis=0, tiled=True)
    rows = lax.all_gather(arrived, "tp", axis=1, tiled=True)
    gate = jnp.dot(rows, w_gate[0], preferred_element_type=F32)
    up = jnp.dot(rows, w_up[0], preferred_element_type=F32)
    hidden = (jax.nn.silu(gate) * up).astype(BF16)
    part = jnp.dot(hidden, w_down[0], preferred_element_type=F32).astype(BF16)
    summed = lax.psum_scatter(part, "tp", scatter_dimension=1, tiled=True)
    back = lax.all_to_all(summed, "ep", split_axis=0, concat_axis=0, tiled=True)
    picked = back[slot].astype(F32).reshape(count, TOP_K, width)
    return jnp.sum(picked * route_weight[:, :, None], axis=1).astype(BF16)


def body(
    direct,
    mix_query,
    forget_input,
    mix_value,
    out_gate_input,
    decay_shift,
    forget_floor,
    head_gain,
    w_mix_out,
    moe_input,
    moe_gain,
    routes,
    route_weight,
    w_exp_gate,
    w_exp_up,
    w_exp_down,
):
    experts = lax.axis_size("ep")
    groups = lax.axis_size("tp")
    me = lax.axis_index("ep").astype(jnp.int32)
    length, width = mix_query.shape
    size = head_gain.shape[0]
    count, depth = moe_input.shape
    slice_width = depth // groups
    cap = -(-5 * count * TOP_K // (4 * experts) // ROWS) * ROWS
    floor = forget_floor.reshape(1, -1)
    head_gain = head_gain.reshape(1, -1)
    half = experts // 2
    near = tuple(range(1, half))
    block = lambda n: ((cap, n), BF16)
    padded = -(-experts // ROWS) * ROWS

    if direct:
        marks = ((padded, count), F32)
        *sent, normed, rank, mark = call(
            functools.partial(spread_body, half),
            [block(depth // 2)] * (half // 2)
            + [((groups, count, slice_width), BF16), marks, marks],
            in_hbm(routes.T, moe_input, moe_gain.reshape(1, -1)),
            LONG,
        )
        far_in = [send(a, half, i) for i, a in enumerate(sent)]
        *near_rows, own_rows = call(
            functools.partial(spread_near_body, near),
            [block(depth // 2)] * len(near) + [block(depth)],
            [normed, rank, mark],
            0,
        )
        near_out = dict(zip(near, near_rows))
        near_in = {}

    state_shape = ((size + ROWS, width), BF16)
    wide_shape = ((cap + size // 2 + ROWS, 2 * width), BF16)
    total, qd, within = call(
        local_body,
        [
            wide_shape if direct else state_shape,
            ((length, width), BF16),
            ((length, width), F32),
        ],
        [mix_query, forget_input, mix_value, decay_shift.T, floor]
        + ([near_out[1]] if direct else []),
        LONG,
    )
    if direct:
        before = []
        bit = 1
        while bit < half:
            near_in[bit] = swap(total, "ep", experts, bit)
            last = 2 * bit == half
            total, *before = call(
                functools.partial(scan_body, bit, not before, cap),
                [state_shape if last else wide_shape, state_shape],
                [total, near_in[bit]] + before + ([] if last else [near_out[2 * bit]]),
                8 * size * width,
            )
            bit *= 2
        for k in near:
            if k not in near_in:
                near_in[k] = swap(near_out[k], "ep", experts, k)

    own_half = lambda at: (at & 1, 2 + (at & 1))
    other_half = lambda at: (1 - (at & 1), 3 - (at & 1))
    everything = lambda at: tuple(range(groups))
    own_plane = lambda at: (at // 2 * 2, at // 2 * 2 + 1)
    other_plane = lambda at: (2 - at // 2 * 2, 3 - at // 2 * 2)
    zero, one = (lambda at: 0), (lambda at: 1)
    own_core, other_core = (lambda at: at & 1), (lambda at: 1 - (at & 1))

    def gathered(i):
        if i == 0:
            here = near_in[1]
            pieces = [own_rows, here, swap(here, "tp", groups, 1)]
            return pieces, [(zero, 1, everything), (one, 1, own_half), (one, 1, other_half)]
        if i < half // 2:
            here = call(
                pack_body, [((2 * cap, depth // 2), BF16)], [near_in[2 * i], near_in[2 * i + 1]], 0
            )[0]
            pieces = [here, swap(here, "tp", groups, 1)]
            return pieces, [(zero, 2, own_half), (zero, 2, other_half)]
        here = far_in[i - half // 2]
        there = swap(here, "tp", groups, 2)
        pieces = [here, there]
        pieces += [swap(here, "tp", groups, 1), swap(there, "tp", groups, 1)]
        return pieces, [
            (own_core, 1, own_plane),
            (own_core, 1, other_plane),
            (other_core, 1, own_plane),
            (other_core, 1, other_plane),
        ]

    if direct:
        weights = (w_exp_gate, w_exp_up, w_exp_down)
        returned, order = [], []
        for i in (0, *range(half // 2, half), *range(1, half // 2)):
            pieces, plan = gathered(i)
            mine, other = expert_call(*weights, pieces, plan, 2, cap)
            got = swap(other, "tp", groups, 1)
            plane = block(depth // 2)
            keep, give = call(halve_body, [plane, plane], [mine, got], 0)
            back = swap(give, "tp", groups, 2)
            done = call(add_body, [plane], [keep, back], 0)[0]
            if i < half // 2:
                order += [2 * i, 2 * i + 1]
                home = send_near(done, experts, i)
            else:
                order += [peer(half, i - half // 2, core) for core in range(2)]
                home = send(done, half, i - half // 2)
            returned += [home, swap(home, "tp", groups, 1)]
        pairs = [(i, i ^ half) for i in range(experts) if not i & half]
        got = lax.ppermute(total, "ep", pairs)
        before = before[0]
        bit = half
    else:
        bit = 0
        before = carried_in(total, me)
        got = before
    head_out = call(
        functools.partial(finish_body, bit),
        [((length, width), BF16)],
        [within, qd, before, got, out_gate_input, head_gain],
        2 * length * size * width,
    )[0]
    if direct:
        across = swap(head_out, "tp", groups, 2)
        pieces = [head_out, across]
        pieces += [swap(head_out, "tp", groups, 1), swap(across, "tp", groups, 1)]
        mixed = call(
            functools.partial(mixed_body, (0, 2, 1, 3)),
            [((length, w_mix_out.shape[1]), BF16)],
            [w_mix_out.reshape(groups, width, -1)] + pieces,
            2 * length * groups * width * w_mix_out.shape[1],
            near=True,
        )[0]
    else:
        mixed = jnp.dot(
            lax.all_gather(head_out, "tp", axis=1, tiled=True),
            w_mix_out,
            preferred_element_type=F32,
        ).astype(BF16)
        moe_out = experts_grouped(
            moe_input, moe_gain, routes, route_weight, w_exp_gate, w_exp_up, w_exp_down
        )
        return (mixed, moe_out)

    first, second, column = call(
        functools.partial(places_body, order, padded),
        [((count, experts * cap), BF16)] * TOP_K + [((count, 8), F32)],
        [routes.T, route_weight.T],
        2 * count * count * padded,
        scratch=[pltpu.VMEM((8, count), F32)],
    )
    seats = [column, first, second]
    part = call(
        functools.partial(combine_body, 0),
        [((count, slice_width), F32)],
        seats + returned[:-2],
        4 * count * experts * cap * slice_width,
        scratch=[pltpu.VMEM(((experts - 2) * cap, slice_width), BF16)],
    )
    moe_out = call(
        functools.partial(combine_body, experts - 2),
        [((count, slice_width), BF16)],
        seats + returned[-2:] + list(part),
        4 * count * 2 * cap * slice_width,
        scratch=[pltpu.VMEM((2 * cap, slice_width), BF16)],
    )[0]
    return (mixed, moe_out)


def solution(mesh):
    placed = (
        P("ep", "tp"),
        P("ep", "tp"),
        P("ep", "tp"),
        P("ep", "tp"),
        P("ep", "tp"),
        P("tp"),
        P(),
        P(None, "tp"),
        P("ep", None),
        P(),
        P("ep", None),
        P("ep", None),
        P("ep", None, "tp"),
        P("ep", None, "tp"),
        P("ep", "tp", None),
    )
    groups = mesh.shape["tp"]
    experts = mesh.shape["ep"]
    direct = groups == 4 and experts <= 8 and experts & (experts - 1) == 0 and experts >= 4

    def whole(*args):
        return body(direct, *args)

    return jax.shard_map(
        whole,
        mesh=mesh,
        in_specs=placed,
        out_specs=(P("ep", "tp"), P("ep", "tp")),
        check_vma=False,
    )
```
